128 devices in a mesh: kv: 16 (over z, y), tp: 8 (over x, core).
Axes of the slice: x: 4, y: 4, z: 4, core: 2. Of those that a mesh axis runs over, the one named last changes fastest.
Arguments:
- tokens: bfloat16 [64, 4096], P(None, 'kv'), may hold values from -170 to 170
- mix_gain: float32 [4096], P('kv'), may hold values from 0.1 to 1.9
- w_query: bfloat16 [4096, 2048], P('kv', 'tp'), may hold values from -0.09375 to 0.09375
- w_key: bfloat16 [4096, 512], P('kv', 'tp'), may hold values from -0.09375 to 0.09375
- w_value: bfloat16 [4096, 512], P('kv', 'tp'), may hold values from -0.09375 to 0.09375
- w_forget: bfloat16 [4096, 32], P('kv', 'tp'), may hold values from -0.09375 to 0.09375
- query_gain: float32 [64], replicated, may hold values from 0.1 to 1.9
- key_cache: bfloat16 [64, 8, 64, 16384], P(None, 'tp', None, 'kv'), may hold values from -1300 to 1300
- value_cache: bfloat16 [64, 8, 64, 16384], P(None, 'tp', None, 'kv'), may hold values from -8 to 8
- decay_cache: float32 [64, 32, 16384], P(None, 'tp', 'kv'), may hold values from -2131.92 to 0, as said below
- w_out: bfloat16 [2048, 4096], P('tp', 'kv'), may hold values from -1 to 1
- mlp_gain: float32 [4096], P('kv'), may hold values from 0.1 to 1.9
- w_up: bfloat16 [4096, 16384], P('kv', 'tp'), may hold values from -0.09375 to 0.09375
- w_down: bfloat16 [16384, 4096], P('tp', 'kv'), may hold values from -0.046875 to 0.046875
Outputs:
- layer_out: bfloat16 [64, 4096], P(None, 'kv')
The draws below stay inside these ranges and needn't reach their ends.
Inputs may be any that keep to these rules, and one draw needn't show every extreme that they name: `decay_cache`: each entry is the sum of the non-positive log forget gates of the later cached positions of its sequence and head: 0 at the last cached position, never smaller at a later position.
All inputs are finite; a program needn't handle non-finite values.
Results may differ from the reference program's by a relative error of at most 0.015.
Values may be sent and summed in bfloat16 or wider, within the bound.
No kernel may reach another device: no remote copies, remote signals or barrier semaphores. Data moves between devices by JAX's collectives and lax.ppermute only.
A program may use at most 64 MiB of HBM per device.

```python
import jax
import jax.numpy as jnp
from jax import lax

D = 4096
HEADS = 32
KV_HEADS = 8
HEAD_DIM = 64
FF = 16384
BATCH = 64
POSITIONS_LOCAL = 1024
POSITIONS = 16384
HEAD_GROUP = 4
FF_GROUP = 2048


def draw_tokens(key, part):
    keys = jax.random.split(key, 2)
    columns = jnp.arange(D, dtype=jnp.float32) / D
    base = jnp.clip(jax.random.normal(keys[0], (BATCH, D), jnp.float32), -4.0, 4.0)
    row_scale = jnp.exp(jax.random.uniform(keys[1], (BATCH, 1), jnp.float32, 0.0, jnp.log(3.0)))
    rising = 3.0 ** columns
    return (base * row_scale * rising[None, :]).astype(jnp.bfloat16)


def draw_key_cache(key, part):
    keys = jax.random.split(key, 3)
    base = jnp.clip(jax.random.normal(keys[0], (BATCH, KV_HEADS, HEAD_DIM, POSITIONS), jnp.float32), -5.0, 5.0)
    low_strength = jnp.log(40.0)
    high_strength = jnp.log(200.0)
    strength = jnp.exp(jax.random.uniform(keys[1], (BATCH, KV_HEADS, 1, 1), jnp.float32, low_strength, high_strength))
    spot = jax.random.randint(keys[2], (BATCH, KV_HEADS, 1, 1), 0, POSITIONS - 1)
    current_location = jnp.arange(POSITIONS).reshape(1, 1, 1, POSITIONS)
    anchor = jnp.take_along_axis(base, jnp.broadcast_to(spot, (BATCH, KV_HEADS, HEAD_DIM, 1)), axis=3)
    bump = jnp.where(current_location == spot + 1, 1.01, 1.0)
    planted = (current_location == spot) | (current_location == spot + 1)
    base = jnp.where(planted, anchor * strength * bump, base)
    return base.astype(jnp.bfloat16)


def draw_value_cache(key, part):
    keys = jax.random.split(key, 2)
    blocks = POSITIONS // POSITIONS_LOCAL
    base = jnp.clip(jax.random.normal(keys[0], (BATCH, KV_HEADS, HEAD_DIM, POSITIONS), jnp.float32), -5.0, 5.0)
    means = jnp.clip(jax.random.normal(keys[1], (BATCH, KV_HEADS, HEAD_DIM, blocks), jnp.float32), -3.0, 3.0)
    return (base + jnp.repeat(means, POSITIONS_LOCAL, axis=3)).astype(jnp.bfloat16)


def draw_decay_cache(key, part):
    keys = jax.random.split(key, 7)
    fast_share = 0.5
    is_fast = jax.random.uniform(keys[0], (BATCH, HEADS, 1), jnp.float32) < fast_share
    slow_rate = jax.random.uniform(keys[1], (BATCH, HEADS, 1), jnp.float32, 0.3, 0.8) / POSITIONS
    fast_rate = jnp.exp(jax.random.uniform(keys[2], (BATCH, HEADS, 1), jnp.float32, jnp.log(0.01), jnp.log(0.04)))
    baseline_rate = jnp.where(is_fast, fast_rate, slow_rate)
    blocks = POSITIONS // POSITIONS_LOCAL
    block_multiplier = jnp.exp(jax.random.uniform(keys[3], (BATCH, HEADS, blocks), jnp.float32, jnp.log(0.5), jnp.log(2.0)))
    coarse_estimate = jax.random.uniform(keys[4], (BATCH, HEADS, POSITIONS), jnp.float32, 0.5, 1.5)
    chosen_places = jax.random.randint(keys[5], (BATCH, HEADS, 2), 0, POSITIONS)
    loss_values = jax.random.uniform(keys[6], (BATCH, HEADS, 2), jnp.float32, 0.22, 0.69)
    current_location = jnp.arange(POSITIONS).reshape(1, 1, POSITIONS)
    sudden_jump = jnp.where(current_location == chosen_places[:, :, 0:1], loss_values[:, :, 0:1], 0.0)
    sudden_jump = sudden_jump + jnp.where(current_location == chosen_places[:, :, 1:2], loss_values[:, :, 1:2], 0.0)
    per_step_rate = baseline_rate * jnp.repeat(block_multiplier, POSITIONS_LOCAL, axis=2) * coarse_estimate + sudden_jump
    after = jnp.flip(jnp.cumsum(jnp.flip(per_step_rate, axis=2), axis=2), axis=2) - per_step_rate
    return -after


def shard_levels(key, extent, cuts, low, high):
    def one(axis_at, blocks):
        draws = jax.random.uniform(jax.random.fold_in(jax.random.fold_in(key, 6), axis_at), (blocks,), jnp.float32, low / len(cuts), high / len(cuts))
        return jnp.repeat(jnp.exp(draws), extent[axis_at] // blocks).reshape((-1,) + (1,) * (len(extent) - axis_at - 1))

    level = one(*cuts[0])
    for cut in cuts[1:]:
        level = level * one(*cut)
    return level


def bell_draw(own_key, dims, scale, limit, shards=(), kind=jnp.bfloat16):
    entries = jax.random.normal(own_key, dims, jnp.float32) * scale
    if len(shards) > 0:
        entries = shard_levels(own_key, dims, shards, -0.22, 0.18) * entries
    return jnp.clip(entries, min=-limit, max=limit).astype(kind)


def setup_inputs(seed: int = 0) -> dict:
    arg_keys = jax.random.split(jax.random.key(seed), 15)
    return {
        "tokens": draw_tokens(jax.random.fold_in(arg_keys[14], 71), 0),
        "mix_gain": jnp.clip(1.0 + 0.18 * jax.random.normal(arg_keys[1], (D,), jnp.float32), 0.1, 1.9),
        "w_query": bell_draw(arg_keys[2], (D, HEADS * HEAD_DIM), D ** -0.5, 0.09375, ((0, 16), (1, 8))),
        "w_key": bell_draw(arg_keys[3], (D, KV_HEADS * HEAD_DIM), D ** -0.5, 0.09375, ((0, 16), (1, 8))),
        "w_value": bell_draw(arg_keys[4], (D, KV_HEADS * HEAD_DIM), D ** -0.5, 0.09375, ((0, 16), (1, 8))),
        "w_forget": bell_draw(arg_keys[5], (D, HEADS), D ** -0.5, 0.09375, ((0, 16), (1, 8))),
        "query_gain": jnp.clip(1.0 + 0.18 * jax.random.normal(arg_keys[6], (HEAD_DIM,), jnp.float32), 0.1, 1.9),
        "key_cache": draw_key_cache(jax.random.fold_in(arg_keys[14], 71), 0),
        "value_cache": draw_value_cache(jax.random.fold_in(arg_keys[14], 71), 0),
        "decay_cache": draw_decay_cache(jax.random.fold_in(arg_keys[14], 71), 0),
        "w_out": bell_draw(arg_keys[10], (HEADS * HEAD_DIM, D), (HEADS * HEAD_DIM // 64) ** -0.5, 1.0, ((0, 8), (1, 16))),
        "mlp_gain": jnp.clip(1.0 + 0.18 * jax.random.normal(arg_keys[11], (D,), jnp.float32), 0.1, 1.9),
        "w_up": bell_draw(arg_keys[12], (D, FF), D ** -0.5, 0.09375, ((0, 16), (1, 8))),
        "w_down": bell_draw(arg_keys[13], (FF, D), FF ** -0.5, 0.046875, ((0, 8), (1, 16))),
    }


EPS = 1e-06

def rounded(value):
    return lax.optimization_barrier(value.astype(jnp.bfloat16)).astype(jnp.float32)

def attend_one(operands):
    query_row, keys_row, values_row, decay_row, forget_row, key_row, value_row = operands
    score_scale = HEAD_DIM ** (-0.5)
    scores = jnp.einsum('gjd,gdp->gjp', query_row.astype(jnp.float32), keys_row.astype(jnp.float32)) * score_scale
    scores = scores + decay_row + forget_row[..., None]
    own_score = jnp.einsum('gjd,gd->gj', query_row.astype(jnp.float32), key_row.astype(jnp.float32)) * score_scale
    peak_score = jnp.maximum(lax.optimization_barrier(jnp.max(scores, axis=-1)), own_score)
    weights = jnp.exp(scores - peak_score[..., None])
    own_weight = jnp.exp(own_score - peak_score)
    totals = lax.optimization_barrier(jnp.sum(weights, axis=-1)) + own_weight
    summed = jnp.einsum('gjp,gdp->gjd', rounded(weights), values_row.astype(jnp.float32))
    summed = summed + rounded(own_weight)[..., None] * value_row.astype(jnp.float32)[:, None, :]
    return summed / totals[..., None]

def reference(tokens, mix_gain, w_query, w_key, w_value, w_forget, query_gain, key_cache, value_cache, decay_cache, w_out, mlp_gain, w_up, w_down):
    stream = tokens.astype(jnp.float32)
    scale_mix = lax.rsqrt(lax.optimization_barrier(jnp.mean(stream * stream, axis=1, keepdims=True)) + EPS)
    normed_mix = (stream * mix_gain.astype(jnp.float32)).astype(jnp.bfloat16)
    query_raw = scale_mix * jnp.dot(normed_mix, w_query, preferred_element_type=jnp.float32)
    key_raw = scale_mix * jnp.dot(normed_mix, w_key, preferred_element_type=jnp.float32)
    value_raw = scale_mix * jnp.dot(normed_mix, w_value, preferred_element_type=jnp.float32)
    forget_raw = scale_mix * jnp.dot(normed_mix, w_forget, preferred_element_type=jnp.float32)
    heads_raw = query_raw.reshape(BATCH, HEADS, HEAD_DIM)
    inverse = lax.rsqrt(lax.optimization_barrier(jnp.mean(heads_raw * heads_raw, axis=-1, keepdims=True)) + EPS)
    query = (heads_raw * inverse * query_gain.astype(jnp.float32)).astype(jnp.bfloat16)
    sharing = HEADS // KV_HEADS
    query = query.reshape(BATCH, KV_HEADS, sharing, HEAD_DIM)
    key_new = key_raw.reshape(BATCH, KV_HEADS, HEAD_DIM).astype(jnp.bfloat16)
    value_new = value_raw.reshape(BATCH, KV_HEADS, HEAD_DIM).astype(jnp.bfloat16)
    log_forget = jax.nn.log_sigmoid(forget_raw).reshape(BATCH, KV_HEADS, sharing)
    decay = decay_cache.reshape(BATCH, KV_HEADS, sharing, -1)
    head_output = lax.map(attend_one, (query, key_cache, value_cache, decay, log_forget, key_new, value_new))
    attended = head_output.reshape(BATCH, HEADS * HEAD_DIM).astype(jnp.bfloat16)
    group_count = HEADS // HEAD_GROUP
    head_width = HEAD_GROUP * HEAD_DIM
    partials = jnp.einsum('bgk,gkd->bgd', attended.reshape(BATCH, group_count, head_width).astype(jnp.float32), w_out.reshape(group_count, head_width, D).astype(jnp.float32))
    attn_out = lax.optimization_barrier(jnp.sum(rounded(partials), axis=1))
    residual = (stream + rounded(attn_out)).astype(jnp.bfloat16)
    residual_wide = residual.astype(jnp.float32)
    scale_mlp = lax.rsqrt(lax.optimization_barrier(jnp.mean(residual_wide * residual_wide, axis=1, keepdims=True)) + EPS)
    normed_mlp = (residual_wide * mlp_gain.astype(jnp.float32)).astype(jnp.bfloat16)
    up_proj = scale_mlp * jnp.dot(normed_mlp, w_up, preferred_element_type=jnp.float32)
    hidden = jnp.square(jax.nn.relu(up_proj)).astype(jnp.bfloat16)
    unit_groups = FF // FF_GROUP
    down_parts = jnp.einsum('bgk,gkd->bgd', hidden.reshape(BATCH, unit_groups, FF_GROUP).astype(jnp.float32), w_down.reshape(unit_groups, FF_GROUP, D).astype(jnp.float32))
    mlp_out = lax.optimization_barrier(jnp.sum(rounded(down_parts), axis=1))
    return (residual_wide + rounded(mlp_out)).astype(jnp.bfloat16)
```

```python
import functools

import jax
import jax.numpy as jnp
from jax import lax
from jax.experimental import pallas as pl
from jax.experimental.pallas import tpu as pltpu
from jax.sharding import PartitionSpec as P

D = 4096
HEAD_DIM = 64
EPS = 1e-06
BF = jnp.bfloat16
F32 = jnp.float32

VM = pl.BlockSpec(memory_space=pltpu.VMEM)
ANY = pl.BlockSpec(memory_space=pl.ANY)


def iota(shape, dim):
    return lax.broadcasted_iota(jnp.int32, shape, dim)


def dot(a, b):
    return jnp.dot(a, b, preferred_element_type=F32)


def dot_t(a, b):
    return lax.dot_general(a, b, (((1,), (1,)), ((), ())), preferred_element_type=F32)


def high(a):
    return a.astype(BF).astype(F32)


def column_to_row(column, width, at):
    n = column.shape[0]
    place = iota((n, width), 1) == iota((n, width), 0) + at
    return jnp.sum(jnp.where(place, column, 0.0), axis=0, keepdims=True)


def row_to_column(row, n, at):
    width = row.shape[1]
    place = iota((n, width), 1) == iota((n, width), 0) + at
    return jnp.sum(jnp.where(place, row, 0.0), axis=1, keepdims=True)


def call(kernel, outs, name, scratch=(), in_specs=None, limit=16 << 20):
    def run(*args):
        return pl.pallas_call(
            kernel,
            out_shape=outs,
            in_specs=in_specs or [VM] * len(args),
            out_specs=jax.tree.map(lambda _: VM, outs),
            scratch_shapes=list(scratch),
            compiler_params=pltpu.CompilerParams(vmem_limit_bytes=limit),
            name=name,
        )(*args)

    return run


def project_kernel(tokens, gain, w_query, w_key, w_value, w_forget, out):
    stream = tokens[...].astype(F32)
    squares = jnp.sum(stream * stream, axis=1, keepdims=True)
    normed = (stream * gain[...]).astype(BF)
    query = dot(normed, w_query[...]).astype(BF)
    key_value = dot_t(normed, jnp.concatenate([w_key[...], w_value[...]], axis=0))
    forget_w = w_forget[...].astype(F32)
    forget_w = jnp.concatenate([forget_w, forget_w, jnp.zeros((120, 256), F32)], axis=0)
    forget = dot_t(normed, forget_w.astype(BF))
    forget = jnp.where(iota(forget.shape, 1) < 4, high(forget), forget - high(forget))
    squares_high = high(squares)
    row_high = column_to_row(squares_high, 128, 64)
    row_low = column_to_row(squares - squares_high, 128, 64)
    line = iota((8, 128), 0)
    square_tile = jnp.where(line == 0, row_high, jnp.where(line == 1, row_low, 0.0))
    for p in range(16):
        t = p // 2
        out[p, 0:64, :] = query
        out[p, 64:72, 0:128] = key_value[8 * t : 8 * t + 8].astype(BF)
        out[p, 64:72, 128:256] = (forget[8 * t : 8 * t + 8] + square_tile).astype(BF)


def attend_kernel(
    parts, query_gain, key_hbm, value_hbm, decay_hbm, out,
    keys, values, decay, key_sem, value_sem, decay_sem, scales, query_rows, left, peaks, masses, sums,
):
    copies = []
    for g in range(8):
        rows = pl.ds(512 * g, 512)
        k_copy = pltpu.make_async_copy(key_hbm.at[rows], keys.at[g], key_sem.at[g])
        d_copy = pltpu.make_async_copy(decay_hbm.at[pl.ds(8 * g, 8)], decay.at[g], decay_sem.at[g])
        v_copy = pltpu.make_async_copy(value_hbm.at[rows], values.at[g], value_sem.at[g])
        k_copy.start()
        d_copy.start()
        v_copy.start()
        copies.append((k_copy, d_copy, v_copy))

    raw = parts[0, 0:64, :].astype(F32)
    extra = parts[0, 64:72, :].astype(F32)
    for i in range(1, 16):
        raw = raw + parts[i, 0:64, :].astype(F32)
        extra = extra + parts[i, 64:72, :].astype(F32)
    squares = row_to_column(extra[0:1, 128:256] + extra[1:2, 128:256], 64, 64)
    scale = lax.rsqrt(squares / D + EPS)
    scales[...] = jnp.broadcast_to(scale, (64, 128))
    heads = scale * raw
    head_of = iota((64, 256), 1) // HEAD_DIM
    power = heads * heads
    inverse = jnp.zeros((64, 256), F32)
    for h in range(4):
        mean = jnp.sum(jnp.where(head_of == h, power, 0.0), axis=1, keepdims=True) / HEAD_DIM
        inverse = jnp.where(head_of == h, lax.rsqrt(mean + EPS), inverse)
    gain = query_gain[...]
    gain = jnp.concatenate([gain, gain, gain, gain], axis=1)
    query = (heads * inverse * gain).astype(BF)

    repeat = (iota((256, 64), 0) // 4 == iota((256, 64), 1)).astype(BF)
    spread = dot(repeat, query)
    own_lanes = iota((256, 256), 1) // HEAD_DIM == iota((256, 256), 0) % 4
    spread = jnp.where(own_lanes, spread, 0.0)
    folded = spread[:, 0:128] + spread[:, 128:256]
    folded = folded + pltpu.roll(folded, 64, 1)
    query_rows[...] = folded
    wide = jnp.concatenate([folded] * 4, axis=1)
    block = iota((256, 512), 1) // HEAD_DIM == (iota((256, 512), 0) // 4) % 8
    left[...] = jnp.where(block, wide, 0.0).astype(BF)

    diagonal = iota((32, 512), 1) // HEAD_DIM == iota((32, 512), 0) // 4
    for g in range(8):
        k_copy, d_copy, v_copy = copies[g]
        rows = slice(32 * g, 32 * g + 32)
        k_copy.wait()
        scores = dot(left[rows, :], keys[g]) * (HEAD_DIM ** (-0.5))
        d_copy.wait()
        scores = scores + decay[g].reshape(32, 1024)
        peak = jnp.max(scores, axis=1, keepdims=True)
        weights = jnp.exp(scores - peak)
        mass = jnp.sum(weights, axis=1, keepdims=True)
        v_copy.wait()
        summed = dot_t(weights.astype(BF), values[g])
        summed = jnp.where(diagonal, summed, 0.0)
        summed = (summed[:, 0:128] + summed[:, 128:256]) + (summed[:, 256:384] + summed[:, 384:512])
        sums[rows, :] = summed + pltpu.roll(summed, 64, 1)
        peaks[rows, :] = jnp.broadcast_to(peak, (32, 128))
        masses[rows, :] = jnp.broadcast_to(mass, (32, 128))

    me = lax.axis_index("kv")
    tile = me // 2
    own_scale = scales[pl.ds(pl.multiple_of(8 * tile, 8), 8), :]
    key_value = (own_scale * extra[:, 0:128]).astype(BF)
    forget = extra[:, 128:256]
    forget = own_scale * (forget + pltpu.roll(forget, 124, 1))
    log_forget = -(jnp.maximum(-forget, 0.0) + jnp.log1p(jnp.exp(-jnp.abs(forget))))
    log_forget = jnp.where(iota((8, 128), 1) < 4, log_forget, 0.0)
    repeat8 = iota((32, 8), 0) // 4 == iota((32, 8), 1)
    key_value = dot(repeat8.astype(BF), key_value)
    log_forget = jnp.dot(
        repeat8.astype(F32), log_forget, preferred_element_type=F32, precision=lax.Precision.HIGHEST
    )
    mine = iota((32, 128), 1) == iota((32, 128), 0) % 4
    log_forget = jnp.sum(jnp.where(mine, log_forget, 0.0), axis=1, keepdims=True)
    at = pl.ds(pl.multiple_of(32 * tile, 32), 32)
    lower = iota((32, 128), 1) < 64
    own = jnp.sum(jnp.where(lower, query_rows[at, :] * key_value, 0.0), axis=1, keepdims=True)
    own = own * (HEAD_DIM ** (-0.5)) - log_forget
    value = jnp.where(lower, pltpu.roll(key_value, 64, 1), key_value)
    peak = peaks[at, :]
    own = jnp.where(me % 2 == 0, jnp.broadcast_to(own, (32, 128)), peak - 1e30)
    top = jnp.maximum(peak, own)
    keep = jnp.exp(peak - top)
    weight = jnp.exp(own - top)
    peaks[at, :] = top
    masses[at, :] = masses[at, :] * keep + weight
    sums[at, :] = sums[at, :] * keep + high(weight) * value

    mass = masses[...]
    level = peaks[...] + jnp.log(mass)
    result = sums[...] / mass
    first = iota((128, 128), 1) < 64
    out[0:128, :] = jnp.where(first, result[0:128], result[128:256]).astype(BF)
    place = iota((128, 128), 0) == iota((128, 128), 1)
    line = iota((8, 128), 0)
    packed = jnp.zeros((8, 128), F32)
    for j in range(2):
        row = jnp.sum(jnp.where(place, level[128 * j : 128 * j + 128], 0.0), axis=0, keepdims=True)
        for k in range(3):
            piece = high(row)
            packed = jnp.where(line == 3 * j + k, piece, packed)
            row = row - piece
    out[128:136, :] = packed.astype(BF)


def merge_kernel(parts, w_out, out):
    extra = parts[:, 128:136, :].astype(F32)
    factors = []
    for j in range(2):
        level = extra[:, 3 * j, :] + extra[:, 3 * j + 1, :] + extra[:, 3 * j + 2, :]
        weight = jnp.exp(level - jnp.max(level, axis=0, keepdims=True))
        factors.append(weight / jnp.sum(weight, axis=0, keepdims=True))
    factors = jnp.concatenate(factors + [jnp.zeros((96, 128), F32)], axis=0).T
    first = iota((128, 128), 1) < 64
    total = jnp.zeros((128, 128), F32)
    for i in range(16):
        factor = jnp.where(first, factors[:, i : i + 1], factors[:, 16 + i : 17 + i])
        total = total + parts[i, 0:128, :].astype(F32) * factor
    turned = pltpu.roll(total, 64, 1)
    own_lanes = iota((128, 256), 1) // HEAD_DIM == iota((128, 256), 0) % 4
    gather = (iota((32, 128), 1) // 4 == iota((32, 128), 0)).astype(BF)
    attended = []
    for j in range(2):
        half = jnp.where(first, total, turned) if j == 0 else jnp.where(first, turned, total)
        half = jnp.where(own_lanes, jnp.concatenate([half, half], axis=1), 0.0).astype(BF)
        attended.append(dot(gather, half))
    attended = jnp.concatenate(attended, axis=0).astype(BF)
    partial = dot(attended, w_out[...]).astype(BF)
    for i in range(8):
        out[i] = partial


def up_kernel(parts, tokens, gain, w_up, residual_out, out):
    attn = parts[0].astype(F32)
    for i in range(1, 8):
        attn = attn + parts[i].astype(F32)
    residual = (tokens[...].astype(F32) + high(attn)).astype(BF)
    residual_out[...] = residual
    wide = residual.astype(F32)
    squares = jnp.sum(wide * wide, axis=1, keepdims=True)
    squares_high = high(squares)
    row_high = column_to_row(squares_high, 128, 0)
    row_low = column_to_row(squares - squares_high, 128, 0)
    line = iota((8, 128), 0)
    tile = jnp.where(line == 0, row_high, jnp.where(line == 1, row_low, 0.0)).astype(BF)
    normed = (wide * gain[...]).astype(BF)
    for p in range(0, 16, 2):
        up = dot(normed, w_up[:, 128 * p : 128 * p + 256]).astype(BF)
        for k in range(2):
            out[p + k, 0:64, :] = up[:, 128 * k : 128 * k + 128]
            out[p + k, 64:72, :] = tile


def hidden_kernel(parts, out):
    up = parts[0, 0:64, :].astype(F32)
    extra = parts[0, 64:72, :].astype(F32)
    for i in range(1, 16):
        up = up + parts[i, 0:64, :].astype(F32)
        extra = extra + parts[i, 64:72, :].astype(F32)
    squares = row_to_column(extra[0:1] + extra[1:2], 64, 0)
    up = lax.rsqrt(squares / D + EPS) * up
    up = jnp.maximum(up, 0.0)
    hidden = (up * up).astype(BF)
    for i in range(16):
        out[i] = hidden


def down_kernel(parts, w_down, out):
    down = jnp.zeros((64, 256), F32)
    for i in range(0, 16, 2):
        pair = jnp.concatenate([parts[i], parts[i + 1]], axis=1)
        down = down + dot(pair, w_down[128 * i : 128 * i + 256, :])
    down = down.astype(BF)
    for i in range(8):
        out[i] = down


def finish_kernel(parts, residual, out):
    down = parts[0].astype(F32)
    for i in range(1, 8):
        down = down + parts[i].astype(F32)
    out[...] = (residual[...].astype(F32) + high(down)).astype(BF)


def exchange(array, axis):
    return lax.all_to_all(array, axis, split_axis=0, concat_axis=0, tiled=True)


def sent(array, axis):
    return exchange(jnp.broadcast_to(array, (lax.axis_size(axis), *array.shape)), axis)


def shards(
    tokens, mix_gain, w_query, w_key, w_value, w_forget, query_gain,
    key_cache, value_cache, decay_cache, w_out, mlp_gain, w_up, w_down,
):
    shape = jax.ShapeDtypeStruct
    message = call(project_kernel, shape((16, 72, 256), BF), "project")(
        tokens, mix_gain.reshape(1, -1), w_query, w_key.T, w_value.T, w_forget.T
    )
    message = exchange(message, "kv")
    part = call(
        attend_kernel,
        shape((136, 128), BF),
        "attend",
        scratch=[
            pltpu.VMEM((8, 512, 1024), BF),
            pltpu.VMEM((8, 512, 1024), BF),
            pltpu.VMEM((8, 8, 4, 1024), F32),
            pltpu.SemaphoreType.DMA((8,)),
            pltpu.SemaphoreType.DMA((8,)),
            pltpu.SemaphoreType.DMA((8,)),
            pltpu.VMEM((64, 128), F32),
            pltpu.VMEM((256, 128), F32),
            pltpu.VMEM((256, 512), BF),
            pltpu.VMEM((256, 128), F32),
            pltpu.VMEM((256, 128), F32),
            pltpu.VMEM((256, 128), F32),
        ],
        in_specs=[VM, VM, ANY, ANY, ANY],
        limit=40 << 20,
    )(
        message,
        query_gain.reshape(1, -1),
        key_cache.reshape(4096, 1024),
        value_cache.reshape(4096, 1024),
        decay_cache,
    )
    message = call(merge_kernel, shape((8, 64, 256), BF), "merge")(sent(part, "kv"), w_out)
    residual, message = call(up_kernel, (shape((64, 256), BF), shape((16, 72, 128), BF)), "up")(
        exchange(message, "tp"), tokens, mlp_gain.reshape(1, -1), w_up
    )
    message = call(hidden_kernel, shape((16, 64, 128), BF), "hidden")(exchange(message, "kv"))
    message = call(down_kernel, shape((8, 64, 256), BF), "down")(exchange(message, "kv"), w_down)
    return call(finish_kernel, shape((64, 256), BF), "finish")(exchange(message, "tp"), residual)


def solution(mesh):
    return jax.shard_map(
        shards,
        mesh=mesh,
        in_specs=(
            P(None, "kv"),
            P("kv"),
            P("kv", "tp"),
            P("kv", "tp"),
            P("kv", "tp"),
            P("kv", "tp"),
            P(),
            P(None, "tp", None, "kv"),
            P(None, "tp", None, "kv"),
            P(None, "tp", "kv"),
            P("tp", "kv"),
            P("kv"),
            P("kv", "tp"),
            P("tp", "kv"),
        ),
        out_specs=P(None, "kv"),
        check_vma=False,
    )
```

```python
import functools

import jax
import jax.numpy as jnp
from jax import lax
from jax.experimental import pallas as pl
from jax.experimental.pallas import tpu as pltpu
from jax.sharding import PartitionSpec as P

D = 4096
HEAD_DIM = 64
EPS = 1e-06
BF = jnp.bfloat16
F32 = jnp.float32

VM = pl.BlockSpec(memory_space=pltpu.VMEM)
HBM = pl.BlockSpec(memory_space=pltpu.HBM)


def iota(shape, dim):
    return lax.broadcasted_iota(jnp.int32, shape, dim)


def dot(a, b):
    return jnp.dot(a, b, preferred_element_type=F32)


def dot_t(a, b):
    return lax.dot_general(a, b, (((1,), (1,)), ((), ())), preferred_element_type=F32)


def high(a):
    return a.astype(BF).astype(F32)


def column_to_row(column, width, at):
    n = column.shape[0]
    place = iota((n, width), 1) == iota((n, width), 0) + at
    return jnp.sum(jnp.where(place, column, 0.0), axis=0, keepdims=True)


def row_to_column(row, n, at):
    width = row.shape[1]
    place = iota((n, width), 1) == iota((n, width), 0) + at
    return jnp.sum(jnp.where(place, row, 0.0), axis=1, keepdims=True)


def call(kernel, outs, name, scratch=(), in_specs=None, limit=16 << 20, cost=None):
    def run(*args):
        return pl.pallas_call(
            kernel,
            out_shape=outs,
            in_specs=in_specs or [VM] * len(args),
            out_specs=jax.tree.map(lambda _: VM, outs),
            scratch_shapes=list(scratch),
            compiler_params=pltpu.CompilerParams(vmem_limit_bytes=limit),
            name=name,
            cost_estimate=cost and pl.CostEstimate(flops=cost, bytes_accessed=cost // 100, transcendentals=0),
        )(*args)

    return run


def project_kernel(*refs):
    sources, (query_out, extra_out), held, sem = refs[:6], refs[6:8], refs[8:14], refs[14]
    copies = [pltpu.make_async_copy(s, h, sem.at[k]) for k, (s, h) in enumerate(zip(sources, held))]
    for copy in copies:
        copy.start()
    for copy in copies:
        copy.wait()
    tokens, gain, w_query, w_key, w_value, w_forget = held
    stream = tokens[...].astype(F32)
    squares = jnp.sum(stream * stream, axis=1, keepdims=True)
    normed = (stream * gain[...]).astype(BF)
    query_out[...] = dot(normed, w_query[...]).astype(BF)
    key_value = dot_t(normed, jnp.concatenate([w_key[...], w_value[...]], axis=0))
    forget_w = w_forget[...].astype(F32)
    forget_w = jnp.concatenate([forget_w, forget_w, jnp.zeros((120, 256), F32)], axis=0)
    forget = dot_t(normed, forget_w.astype(BF))
    forget = jnp.where(iota(forget.shape, 1) < 4, high(forget), forget - high(forget))
    squares_high = high(squares)
    row_high = column_to_row(squares_high, 128, 64)
    row_low = column_to_row(squares - squares_high, 128, 64)
    line = iota((64, 128), 0) % 8
    forget = forget + jnp.where(line == 0, row_high, jnp.where(line == 1, row_low, 0.0))
    extra_out[:, 0:128] = key_value.astype(BF)
    extra_out[:, 128:256] = forget.astype(BF)


def spread_kernel(query, extra, out):
    for p in range(16):
        out[p, 0:64, :] = query[...]
        out[p, 64:72, :] = extra[8 * (p // 2) : 8 * (p // 2) + 8, :]


def attend_kernel(
    parts, query_gain, keys, values, decay, out,
    scales, query_rows, left, peaks, masses, sums,
):
    raw = parts[0, 0:64, :].astype(F32)
    extra = parts[0, 64:72, :].astype(F32)
    for i in range(1, 16):
        raw = raw + parts[i, 0:64, :].astype(F32)
        extra = extra + parts[i, 64:72, :].astype(F32)
    squares = row_to_column(extra[0:1, 128:256] + extra[1:2, 128:256], 64, 64)
    scale = lax.rsqrt(squares / D + EPS)
    scales[...] = jnp.broadcast_to(scale, (64, 128))
    heads = scale * raw
    head_of = iota((64, 256), 1) // HEAD_DIM
    power = heads * heads
    inverse = jnp.zeros((64, 256), F32)
    for h in range(4):
        mean = jnp.sum(jnp.where(head_of == h, power, 0.0), axis=1, keepdims=True) / HEAD_DIM
        inverse = jnp.where(head_of == h, lax.rsqrt(mean + EPS), inverse)
    gain = query_gain[...]
    gain = jnp.concatenate([gain, gain, gain, gain], axis=1)
    query = (heads * inverse * gain).astype(BF)

    repeat = (iota((256, 64), 0) // 4 == iota((256, 64), 1)).astype(BF)
    spread = dot(repeat, query)
    own_lanes = iota((256, 256), 1) // HEAD_DIM == iota((256, 256), 0) % 4
    spread = jnp.where(own_lanes, spread, 0.0)
    folded = spread[:, 0:128] + spread[:, 128:256]
    folded = folded + pltpu.roll(folded, 64, 1)
    query_rows[...] = folded
    wide = jnp.concatenate([folded] * 4, axis=1)
    block = iota((256, 512), 1) // HEAD_DIM == (iota((256, 512), 0) // 4) % 8
    left[...] = jnp.where(block, wide, 0.0).astype(BF)

    diagonal = iota((32, 512), 1) // HEAD_DIM == iota((32, 512), 0) // 4
    for g in range(8):
        rows = slice(32 * g, 32 * g + 32)
        scores = dot(left[rows, :], keys[512 * g : 512 * g + 512, :]) * (HEAD_DIM ** (-0.5))
        scores = scores + decay[8 * g : 8 * g + 8].reshape(32, 1024)
        peak = jnp.max(scores, axis=1, keepdims=True)
        weights = jnp.exp(scores - peak)
        mass = jnp.sum(weights, axis=1, keepdims=True)
        summed = dot_t(weights.astype(BF), values[512 * g : 512 * g + 512, :])
        summed = jnp.where(diagonal, summed, 0.0)
        summed = (summed[:, 0:128] + summed[:, 128:256]) + (summed[:, 256:384] + summed[:, 384:512])
        sums[rows, :] = summed + pltpu.roll(summed, 64, 1)
        peaks[rows, :] = jnp.broadcast_to(peak, (32, 128))
        masses[rows, :] = jnp.broadcast_to(mass, (32, 128))

    me = lax.axis_index("kv")
    tile = me // 2
    own_scale = scales[pl.ds(pl.multiple_of(8 * tile, 8), 8), :]
    key_value = (own_scale * extra[:, 0:128]).astype(BF)
    forget = extra[:, 128:256]
    forget = own_scale * (forget + pltpu.roll(forget, 124, 1))
    log_forget = -(jnp.maximum(-forget, 0.0) + jnp.log1p(jnp.exp(-jnp.abs(forget))))
    log_forget = jnp.where(iota((8, 128), 1) < 4, log_forget, 0.0)
    repeat8 = iota((32, 8), 0) // 4 == iota((32, 8), 1)
    key_value = dot(repeat8.astype(BF), key_value)
    log_forget = jnp.dot(
        repeat8.astype(F32), log_forget, preferred_element_type=F32, precision=lax.Precision.HIGHEST
    )
    mine = iota((32, 128), 1) == iota((32, 128), 0) % 4
    log_forget = jnp.sum(jnp.where(mine, log_forget, 0.0), axis=1, keepdims=True)
    at = pl.ds(pl.multiple_of(32 * tile, 32), 32)
    lower = iota((32, 128), 1) < 64
    own = jnp.sum(jnp.where(lower, query_rows[at, :] * key_value, 0.0), axis=1, keepdims=True)
    own = own * (HEAD_DIM ** (-0.5)) - log_forget
    value = jnp.where(lower, pltpu.roll(key_value, 64, 1), key_value)
    peak = peaks[at, :]
    own = jnp.where(me % 2 == 0, jnp.broadcast_to(own, (32, 128)), peak - 1e30)
    top = jnp.maximum(peak, own)
    keep = jnp.exp(peak - top)
    weight = jnp.exp(own - top)
    peaks[at, :] = top
    masses[at, :] = masses[at, :] * keep + weight
    sums[at, :] = sums[at, :] * keep + high(weight) * value

    mass = masses[...]
    level = peaks[...] + jnp.log(mass)
    result = sums[...] / mass
    first = iota((128, 128), 1) < 64
    out[0:128, :] = jnp.where(first, result[0:128], result[128:256]).astype(BF)
    place = iota((128, 128), 0) == iota((128, 128), 1)
    line = iota((8, 128), 0)
    packed = jnp.zeros((8, 128), F32)
    for j in range(2):
        row = jnp.sum(jnp.where(place, level[128 * j : 128 * j + 128], 0.0), axis=0, keepdims=True)
        for k in range(3):
            piece = high(row)
            packed = jnp.where(line == 3 * j + k, piece, packed)
            row = row - piece
    out[128:136, :] = packed.astype(BF)


def merge_kernel(parts, w_out, out):
    extra = parts[:, 128:136, :].astype(F32)
    factors = []
    for j in range(2):
        level = extra[:, 3 * j, :] + extra[:, 3 * j + 1, :] + extra[:, 3 * j + 2, :]
        weight = jnp.exp(level - jnp.max(level, axis=0, keepdims=True))
        factors.append(weight / jnp.sum(weight, axis=0, keepdims=True))
    factors = jnp.concatenate(factors + [jnp.zeros((96, 128), F32)], axis=0).T
    first = iota((128, 128), 1) < 64
    total = jnp.zeros((128, 128), F32)
    for i in range(16):
        factor = jnp.where(first, factors[:, i : i + 1], factors[:, 16 + i : 17 + i])
        total = total + parts[i, 0:128, :].astype(F32) * factor
    turned = pltpu.roll(total, 64, 1)
    own_lanes = iota((128, 256), 1) // HEAD_DIM == iota((128, 256), 0) % 4
    gather = (iota((32, 128), 1) // 4 == iota((32, 128), 0)).astype(BF)
    attended = []
    for j in range(2):
        half = jnp.where(first, total, turned) if j == 0 else jnp.where(first, turned, total)
        half = jnp.where(own_lanes, jnp.concatenate([half, half], axis=1), 0.0).astype(BF)
        attended.append(dot(gather, half))
    attended = jnp.concatenate(attended, axis=0).astype(BF)
    partial = dot(attended, w_out[...]).astype(BF)
    for i in range(8):
        out[i] = partial


def up_kernel(parts, tokens, gain, w_up, residual_out, out):
    attn = parts[0].astype(F32)
    for i in range(1, 8):
        attn = attn + parts[i].astype(F32)
    residual = (tokens[...].astype(F32) + high(attn)).astype(BF)
    residual_out[...] = residual
    wide = residual.astype(F32)
    squares = jnp.sum(wide * wide, axis=1, keepdims=True)
    squares_high = high(squares)
    row_high = column_to_row(squares_high, 128, 0)
    row_low = column_to_row(squares - squares_high, 128, 0)
    line = iota((8, 128), 0)
    tile = jnp.where(line == 0, row_high, jnp.where(line == 1, row_low, 0.0)).astype(BF)
    normed = (wide * gain[...]).astype(BF)
    for p in range(0, 16, 2):
        up = dot(normed, w_up[:, 128 * p : 128 * p + 256]).astype(BF)
        for k in range(2):
            out[p + k, 0:64, :] = up[:, 128 * k : 128 * k + 128]
            out[p + k, 64:72, :] = tile


def hidden_kernel(parts, out):
    up = parts[0, 0:64, :].astype(F32)
    extra = parts[0, 64:72, :].astype(F32)
    for i in range(1, 16):
        up = up + parts[i, 0:64, :].astype(F32)
        extra = extra + parts[i, 64:72, :].astype(F32)
    squares = row_to_column(extra[0:1] + extra[1:2], 64, 0)
    up = lax.rsqrt(squares / D + EPS) * up
    up = jnp.maximum(up, 0.0)
    hidden = (up * up).astype(BF)
    for i in range(16):
        out[i] = hidden


def down_kernel(parts, w_down, out):
    down = jnp.zeros((64, 256), F32)
    for i in range(0, 16, 2):
        pair = jnp.concatenate([parts[i], parts[i + 1]], axis=1)
        down = down + dot(pair, w_down[128 * i : 128 * i + 256, :])
    down = down.astype(BF)
    for i in range(8):
        out[i] = down


def finish_kernel(parts, residual, out):
    down = parts[0].astype(F32)
    for i in range(1, 8):
        down = down + parts[i].astype(F32)
    out[...] = (residual[...].astype(F32) + high(down)).astype(BF)


def exchange(array, axis):
    return lax.all_to_all(array, axis, split_axis=0, concat_axis=0, tiled=True)


def sent(array, axis):
    return exchange(jnp.broadcast_to(array, (lax.axis_size(axis), *array.shape)), axis)


def shards(
    tokens, mix_gain, w_query, w_key, w_value, w_forget, query_gain,
    key_cache, value_cache, decay_cache, w_out, mlp_gain, w_up, w_down,
):
    shape = jax.ShapeDtypeStruct
    query, extra = call(
        project_kernel,
        (shape((64, 256), BF), shape((64, 256), BF)),
        "project",
        scratch=[
            pltpu.VMEM((64, 256), BF),
            pltpu.VMEM((1, 256), F32),
            pltpu.VMEM((256, 256), BF),
            pltpu.VMEM((64, 256), BF),
            pltpu.VMEM((64, 256), BF),
            pltpu.VMEM((4, 256), BF),
            pltpu.SemaphoreType.DMA((6,)),
        ],
        in_specs=[HBM] * 6,
    )(tokens, mix_gain.reshape(1, -1), w_query, w_key.T, w_value.T, w_forget.T)
    message = call(spread_kernel, shape((16, 72, 256), BF), "spread", cost=10**10)(query, extra)
    message = exchange(message, "kv")
    part = call(
        attend_kernel,
        shape((136, 128), BF),
        "attend",
        scratch=[
            pltpu.VMEM((64, 128), F32),
            pltpu.VMEM((256, 128), F32),
            pltpu.VMEM((256, 512), BF),
            pltpu.VMEM((256, 128), F32),
            pltpu.VMEM((256, 128), F32),
            pltpu.VMEM((256, 128), F32),
        ],

        limit=8 << 20,
    )(
        message,
        query_gain.reshape(1, -1),
        key_cache.reshape(4096, 1024),
        value_cache.reshape(4096, 1024),
        decay_cache,
    )
    message = call(merge_kernel, shape((8, 64, 256), BF), "merge")(sent(part, "kv"), w_out)
    residual, message = call(up_kernel, (shape((64, 256), BF), shape((16, 72, 128), BF)), "up")(
        exchange(message, "tp"), tokens, mlp_gain.reshape(1, -1), w_up
    )
    message = call(hidden_kernel, shape((16, 64, 128), BF), "hidden")(exchange(message, "kv"))
    message = call(down_kernel, shape((8, 64, 256), BF), "down")(exchange(message, "kv"), w_down)
    return call(finish_kernel, shape((64, 256), BF), "finish")(exchange(message, "tp"), residual)


def solution(mesh):
    return jax.shard_map(
        shards,
        mesh=mesh,
        in_specs=(
            P(None, "kv"),
            P("kv"),
            P("kv", "tp"),
            P("kv", "tp"),
            P("kv", "tp"),
            P("kv", "tp"),
            P(),
            P(None, "tp", None, "kv"),
            P(None, "tp", None, "kv"),
            P(None, "tp", "kv"),
            P("tp", "kv"),
            P("kv"),
            P("kv", "tp"),
            P("tp", "kv"),
        ),
        out_specs=P(None, "kv"),
        check_vma=False,
    )
```

```python
import functools

import jax
import jax.numpy as jnp
from jax import lax
from jax.experimental import pallas as pl
from jax.experimental.pallas import tpu as pltpu
from jax.sharding import PartitionSpec as P

D = 4096
HEAD_DIM = 64
EPS = 1e-06
BF = jnp.bfloat16
F32 = jnp.float32

VM = pl.BlockSpec(memory_space=pltpu.VMEM)


def iota(shape, dim):
    return lax.broadcasted_iota(jnp.int32, shape, dim)


def dot(a, b):
    return jnp.dot(a, b, preferred_element_type=F32)


def dot_t(a, b):
    return lax.dot_general(a, b, (((1,), (1,)), ((), ())), preferred_element_type=F32)


def high(a):
    return a.astype(BF).astype(F32)


def column_to_row(column, width, at):
    n = column.shape[0]
    place = iota((n, width), 1) == iota((n, width), 0) + at
    return jnp.sum(jnp.where(place, column, 0.0), axis=0, keepdims=True)


def row_to_column(row, n, at):
    width = row.shape[1]
    place = iota((n, width), 1) == iota((n, width), 0) + at
    return jnp.sum(jnp.where(place, row, 0.0), axis=1, keepdims=True)


def call(kernel, outs, name, scratch=(), in_specs=None, limit=16 << 20, cost=None):
    def run(*args):
        return pl.pallas_call(
            kernel,
            out_shape=outs,
            in_specs=in_specs or [VM] * len(args),
            out_specs=jax.tree.map(lambda _: VM, outs),
            scratch_shapes=list(scratch),
            compiler_params=pltpu.CompilerParams(vmem_limit_bytes=limit),
            name=name,
            cost_estimate=cost and pl.CostEstimate(flops=cost, bytes_accessed=cost // 100, transcendentals=0),
        )(*args)

    return run


def project_kernel(head, tokens, gain, w_query, w_key, w_value, w_forget, query_out, extra_out):
    stream = tokens[...].astype(F32)
    squares = jnp.sum(stream * stream, axis=1, keepdims=True)
    normed = (stream * gain[...]).astype(BF)
    query_out[...] = dot(normed, w_query[...]).astype(BF)
    key_value = dot_t(normed, jnp.concatenate([w_key[...], w_value[...]], axis=0))
    forget_w = w_forget[...].astype(F32)
    forget_w = jnp.concatenate([forget_w, forget_w, jnp.zeros((120, 256), F32)], axis=0)
    forget = dot_t(normed, forget_w.astype(BF))
    forget = jnp.where(iota(forget.shape, 1) < 4, high(forget), forget - high(forget))
    squares_high = high(squares)
    row_high = column_to_row(squares_high, 128, 64)
    row_low = column_to_row(squares - squares_high, 128, 64)
    line = iota((64, 128), 0) % 8
    forget = forget + jnp.where(line == 0, row_high, jnp.where(line == 1, row_low, 0.0))
    extra_out[:, 0:128] = key_value.astype(BF)
    extra_out[:, 128:256] = forget.astype(BF)


def head_kernel(out):
    out[...] = jnp.zeros_like(out)


def spread_kernel(query, extra, out):
    for p in range(16):
        out[p, 0:64, :] = query[...]
        out[p, 64:72, :] = extra[8 * (p // 2) : 8 * (p // 2) + 8, :]


def attend_kernel(
    parts, query_gain, keys, values, decay, out,
    scales, query_rows, left, peaks, masses, sums,
):
    raw = parts[0, 0:64, :].astype(F32)
    extra = parts[0, 64:72, :].astype(F32)
    for i in range(1, 16):
        raw = raw + parts[i, 0:64, :].astype(F32)
        extra = extra + parts[i, 64:72, :].astype(F32)
    squares = row_to_column(extra[0:1, 128:256] + extra[1:2, 128:256], 64, 64)
    scale = lax.rsqrt(squares / D + EPS)
    scales[...] = jnp.broadcast_to(scale, (64, 128))
    heads = scale * raw
    head_of = iota((64, 256), 1) // HEAD_DIM
    power = heads * heads
    inverse = jnp.zeros((64, 256), F32)
    for h in range(4):
        mean = jnp.sum(jnp.where(head_of == h, power, 0.0), axis=1, keepdims=True) / HEAD_DIM
        inverse = jnp.where(head_of == h, lax.rsqrt(mean + EPS), inverse)
    gain = query_gain[...]
    gain = jnp.concatenate([gain, gain, gain, gain], axis=1)
    query = (heads * inverse * gain).astype(BF)

    repeat = (iota((256, 64), 0) // 4 == iota((256, 64), 1)).astype(BF)
    spread = dot(repeat, query)
    own_lanes = iota((256, 256), 1) // HEAD_DIM == iota((256, 256), 0) % 4
    spread = jnp.where(own_lanes, spread, 0.0)
    folded = spread[:, 0:128] + spread[:, 128:256]
    folded = folded + pltpu.roll(folded, 64, 1)
    query_rows[...] = folded
    wide = jnp.concatenate([folded] * 4, axis=1)
    block = iota((256, 512), 1) // HEAD_DIM == (iota((256, 512), 0) // 4) % 8
    left[...] = jnp.where(block, wide, 0.0).astype(BF)

    diagonal = iota((32, 512), 1) // HEAD_DIM == iota((32, 512), 0) // 4
    for g in range(8):
        rows = slice(32 * g, 32 * g + 32)
        scores = dot(left[rows, :], keys[512 * g : 512 * g + 512, :]) * (HEAD_DIM ** (-0.5))
        scores = scores + decay[8 * g : 8 * g + 8].reshape(32, 1024)
        peak = jnp.max(scores, axis=1, keepdims=True)
        weights = jnp.exp(scores - peak)
        mass = jnp.sum(weights, axis=1, keepdims=True)
        summed = dot_t(weights.astype(BF), values[512 * g : 512 * g + 512, :])
        summed = jnp.where(diagonal, summed, 0.0)
        summed = (summed[:, 0:128] + summed[:, 128:256]) + (summed[:, 256:384] + summed[:, 384:512])
        sums[rows, :] = summed + pltpu.roll(summed, 64, 1)
        peaks[rows, :] = jnp.broadcast_to(peak, (32, 128))
        masses[rows, :] = jnp.broadcast_to(mass, (32, 128))

    me = lax.axis_index("kv")
    tile = me // 2
    own_scale = scales[pl.ds(pl.multiple_of(8 * tile, 8), 8), :]
    key_value = (own_scale * extra[:, 0:128]).astype(BF)
    forget = extra[:, 128:256]
    forget = own_scale * (forget + pltpu.roll(forget, 124, 1))
    log_forget = -(jnp.maximum(-forget, 0.0) + jnp.log1p(jnp.exp(-jnp.abs(forget))))
    log_forget = jnp.where(iota((8, 128), 1) < 4, log_forget, 0.0)
    repeat8 = iota((32, 8), 0) // 4 == iota((32, 8), 1)
    key_value = dot(repeat8.astype(BF), key_value)
    log_forget = jnp.dot(
        repeat8.astype(F32), log_forget, preferred_element_type=F32, precision=lax.Precision.HIGHEST
    )
    mine = iota((32, 128), 1) == iota((32, 128), 0) % 4
    log_forget = jnp.sum(jnp.where(mine, log_forget, 0.0), axis=1, keepdims=True)
    at = pl.ds(pl.multiple_of(32 * tile, 32), 32)
    lower = iota((32, 128), 1) < 64
    own = jnp.sum(jnp.where(lower, query_rows[at, :] * key_value, 0.0), axis=1, keepdims=True)
    own = own * (HEAD_DIM ** (-0.5)) - log_forget
    value = jnp.where(lower, pltpu.roll(key_value, 64, 1), key_value)
    peak = peaks[at, :]
    own = jnp.where(me % 2 == 0, jnp.broadcast_to(own, (32, 128)), peak - 1e30)
    top = jnp.maximum(peak, own)
    keep = jnp.exp(peak - top)
    weight = jnp.exp(own - top)
    peaks[at, :] = top
    masses[at, :] = masses[at, :] * keep + weight
    sums[at, :] = sums[at, :] * keep + high(weight) * value

    mass = masses[...]
    level = peaks[...] + jnp.log(mass)
    result = sums[...] / mass
    first = iota((128, 128), 1) < 64
    out[0:128, :] = jnp.where(first, result[0:128], result[128:256]).astype(BF)
    place = iota((128, 128), 0) == iota((128, 128), 1)
    line = iota((8, 128), 0)
    packed = jnp.zeros((8, 128), F32)
    for j in range(2):
        row = jnp.sum(jnp.where(place, level[128 * j : 128 * j + 128], 0.0), axis=0, keepdims=True)
        for k in range(3):
            piece = high(row)
            packed = jnp.where(line == 3 * j + k, piece, packed)
            row = row - piece
    out[128:136, :] = packed.astype(BF)


def merge_kernel(parts, w_out, out):
    extra = parts[:, 128:136, :].astype(F32)
    factors = []
    for j in range(2):
        level = extra[:, 3 * j, :] + extra[:, 3 * j + 1, :] + extra[:, 3 * j + 2, :]
        weight = jnp.exp(level - jnp.max(level, axis=0, keepdims=True))
        factors.append(weight / jnp.sum(weight, axis=0, keepdims=True))
    factors = jnp.concatenate(factors + [jnp.zeros((96, 128), F32)], axis=0).T
    first = iota((128, 128), 1) < 64
    total = jnp.zeros((128, 128), F32)
    for i in range(16):
        factor = jnp.where(first, factors[:, i : i + 1], factors[:, 16 + i : 17 + i])
        total = total + parts[i, 0:128, :].astype(F32) * factor
    turned = pltpu.roll(total, 64, 1)
    own_lanes = iota((128, 256), 1) // HEAD_DIM == iota((128, 256), 0) % 4
    gather = (iota((32, 128), 1) // 4 == iota((32, 128), 0)).astype(BF)
    attended = []
    for j in range(2):
        half = jnp.where(first, total, turned) if j == 0 else jnp.where(first, turned, total)
        half = jnp.where(own_lanes, jnp.concatenate([half, half], axis=1), 0.0).astype(BF)
        attended.append(dot(gather, half))
    attended = jnp.concatenate(attended, axis=0).astype(BF)
    partial = dot(attended, w_out[...]).astype(BF)
    for i in range(8):
        out[i] = partial


def up_kernel(parts, tokens, gain, w_up, residual_out, out):
    attn = parts[0].astype(F32)
    for i in range(1, 8):
        attn = attn + parts[i].astype(F32)
    residual = (tokens[...].astype(F32) + high(attn)).astype(BF)
    residual_out[...] = residual
    wide = residual.astype(F32)
    squares = jnp.sum(wide * wide, axis=1, keepdims=True)
    squares_high = high(squares)
    row_high = column_to_row(squares_high, 128, 0)
    row_low = column_to_row(squares - squares_high, 128, 0)
    line = iota((8, 128), 0)
    tile = jnp.where(line == 0, row_high, jnp.where(line == 1, row_low, 0.0)).astype(BF)
    normed = (wide * gain[...]).astype(BF)
    for p in range(0, 16, 2):
        up = dot(normed, w_up[:, 128 * p : 128 * p + 256]).astype(BF)
        for k in range(2):
            out[p + k, 0:64, :] = up[:, 128 * k : 128 * k + 128]
            out[p + k, 64:72, :] = tile


def hidden_kernel(parts, out):
    up = parts[0, 0:64, :].astype(F32)
    extra = parts[0, 64:72, :].astype(F32)
    for i in range(1, 16):
        up = up + parts[i, 0:64, :].astype(F32)
        extra = extra + parts[i, 64:72, :].astype(F32)
    squares = row_to_column(extra[0:1] + extra[1:2], 64, 0)
    up = lax.rsqrt(squares / D + EPS) * up
    up = jnp.maximum(up, 0.0)
    hidden = (up * up).astype(BF)
    for i in range(16):
        out[i] = hidden


def down_kernel(parts, w_down, out):
    down = jnp.zeros((64, 256), F32)
    for i in range(0, 16, 2):
        pair = jnp.concatenate([parts[i], parts[i + 1]], axis=1)
        down = down + dot(pair, w_down[128 * i : 128 * i + 256, :])
    down = down.astype(BF)
    for i in range(8):
        out[i] = down


def finish_kernel(parts, residual, out):
    down = parts[0].astype(F32)
    for i in range(1, 8):
        down = down + parts[i].astype(F32)
    out[...] = (residual[...].astype(F32) + high(down)).astype(BF)


def exchange(array, axis):
    return lax.all_to_all(array, axis, split_axis=0, concat_axis=0, tiled=True)


def sent(array, axis):
    return exchange(jnp.broadcast_to(array, (lax.axis_size(axis), *array.shape)), axis)


def shards(
    tokens, mix_gain, w_query, w_key, w_value, w_forget, query_gain,
    key_cache, value_cache, decay_cache, w_out, mlp_gain, w_up, w_down,
):
    shape = jax.ShapeDtypeStruct
    head = call(head_kernel, shape((8, 128), F32), "head", cost=3 * 10**9)()
    operands = (tokens, mix_gain.reshape(1, -1), w_query, w_key.T, w_value.T, w_forget.T)
    query, extra = call(project_kernel, (shape((64, 256), BF), shape((64, 256), BF)), "project")(head, *operands)
    message = call(spread_kernel, shape((16, 72, 256), BF), "spread", cost=10**10)(query, extra)
    message = exchange(message, "kv")
    part = call(
        attend_kernel,
        shape((136, 128), BF),
        "attend",
        scratch=[
            pltpu.VMEM((64, 128), F32),
            pltpu.VMEM((256, 128), F32),
            pltpu.VMEM((256, 512), BF),
            pltpu.VMEM((256, 128), F32),
            pltpu.VMEM((256, 128), F32),
            pltpu.VMEM((256, 128), F32),
        ],

        limit=8 << 20,
    )(
        message,
        query_gain.reshape(1, -1),
        key_cache.reshape(4096, 1024),
        value_cache.reshape(4096, 1024),
        decay_cache,
    )
    message = call(merge_kernel, shape((8, 64, 256), BF), "merge")(sent(part, "kv"), w_out)
    residual, message = call(up_kernel, (shape((64, 256), BF), shape((16, 72, 128), BF)), "up")(
        exchange(message, "tp"), tokens, mlp_gain.reshape(1, -1), w_up
    )
    message = call(hidden_kernel, shape((16, 64, 128), BF), "hidden")(exchange(message, "kv"))
    message = call(down_kernel, shape((8, 64, 256), BF), "down")(exchange(message, "kv"), w_down)
    return call(finish_kernel, shape((64, 256), BF), "finish")(exchange(message, "tp"), residual)


def solution(mesh):
    return jax.shard_map(
        shards,
        mesh=mesh,
        in_specs=(
            P(None, "kv"),
            P("kv"),
            P("kv", "tp"),
            P("kv", "tp"),
            P("kv", "tp"),
            P("kv", "tp"),
            P(),
            P(None, "tp", None, "kv"),
            P(None, "tp", None, "kv"),
            P(None, "tp", "kv"),
            P("tp", "kv"),
            P("kv"),
            P("kv", "tp"),
            P("tp", "kv"),
        ),
        out_specs=P(None, "kv"),
        check_vma=False,
    )
```

```python
import functools

import jax
import jax.numpy as jnp
from jax import lax
from jax.experimental import pallas as pl
from jax.experimental.pallas import tpu as pltpu
from jax.sharding import PartitionSpec as P

D = 4096
HEAD_DIM = 64
EPS = 1e-06
BF = jnp.bfloat16
F32 = jnp.float32

VM = pl.BlockSpec(memory_space=pltpu.VMEM)


def iota(shape, dim):
    return lax.broadcasted_iota(jnp.int32, shape, dim)


def dot(a, b):
    return jnp.dot(a, b, preferred_element_type=F32)


def dot_t(a, b):
    return lax.dot_general(a, b, (((1,), (1,)), ((), ())), preferred_element_type=F32)


def high(a):
    return a.astype(BF).astype(F32)


def column_to_row(column, width, at):
    n = column.shape[0]
    place = iota((n, width), 1) == iota((n, width), 0) + at
    return jnp.sum(jnp.where(place, column, 0.0), axis=0, keepdims=True)


def row_to_column(row, n, at):
    width = row.shape[1]
    place = iota((n, width), 1) == iota((n, width), 0) + at
    return jnp.sum(jnp.where(place, row, 0.0), axis=1, keepdims=True)


def call(kernel, outs, name, scratch=(), in_specs=None, limit=16 << 20, cost=None):
    def run(*args):
        return pl.pallas_call(
            kernel,
            out_shape=outs,
            in_specs=in_specs or [VM] * len(args),
            out_specs=jax.tree.map(lambda _: VM, outs),
            scratch_shapes=list(scratch),
            compiler_params=pltpu.CompilerParams(vmem_limit_bytes=limit),
            name=name,
            cost_estimate=cost and pl.CostEstimate(flops=cost, bytes_accessed=cost // 100, transcendentals=0),
        )(*args)

    return run


def project_kernel(head, tokens, gain, w_query, w_key, w_value, w_forget, query_out, extra_out):
    stream = tokens[...].astype(F32)
    squares = jnp.sum(stream * stream, axis=1, keepdims=True)
    normed = (stream * gain[...]).astype(BF)
    query_out[...] = dot(normed, w_query[...]).astype(BF)
    key_value = dot_t(normed, jnp.concatenate([w_key[...], w_value[...]], axis=0))
    forget_w = w_forget[...].astype(F32)
    forget_w = jnp.concatenate([forget_w, forget_w, jnp.zeros((120, 256), F32)], axis=0)
    forget = dot_t(normed, forget_w.astype(BF))
    forget = jnp.where(iota(forget.shape, 1) < 4, high(forget), forget - high(forget))
    squares_high = high(squares)
    row_high = column_to_row(squares_high, 128, 64)
    row_low = column_to_row(squares - squares_high, 128, 64)
    line = iota((64, 128), 0) % 8
    forget = forget + jnp.where(line == 0, row_high, jnp.where(line == 1, row_low, 0.0))
    extra_out[:, 0:128] = key_value.astype(BF)
    extra_out[:, 128:256] = forget.astype(BF)


def head_kernel(out):
    out[...] = jnp.zeros_like(out)


def spread_kernel(query, extra, out):
    for p in range(16):
        out[p, 0:64, :] = query[...]
        out[p, 64:72, :] = extra[8 * (p // 2) : 8 * (p // 2) + 8, :]


def attend_kernel(
    parts, query_gain, keys, values, decay, out,
    scales, query_rows, left, peaks, masses,
):
    raw = parts[0, 0:64, :].astype(F32)
    extra = parts[0, 64:72, :].astype(F32)
    for i in range(1, 16):
        raw = raw + parts[i, 0:64, :].astype(F32)
        extra = extra + parts[i, 64:72, :].astype(F32)
    squares = row_to_column(extra[0:1, 128:256] + extra[1:2, 128:256], 64, 64)
    scale = lax.rsqrt(squares / D + EPS)
    scales[...] = jnp.broadcast_to(scale, (64, 128))
    heads = scale * raw
    head_of = iota((64, 256), 1) // HEAD_DIM
    power = heads * heads
    inverse = jnp.zeros((64, 256), F32)
    for h in range(4):
        mean = jnp.sum(jnp.where(head_of == h, power, 0.0), axis=1, keepdims=True) / HEAD_DIM
        inverse = jnp.where(head_of == h, lax.rsqrt(mean + EPS), inverse)
    gain = query_gain[...]
    gain = jnp.concatenate([gain, gain, gain, gain], axis=1)
    query = (heads * inverse * gain).astype(BF)

    repeat = (iota((256, 64), 0) // 4 == iota((256, 64), 1)).astype(BF)
    spread = dot(repeat, query)
    own_lanes = iota((256, 256), 1) // HEAD_DIM == iota((256, 256), 0) % 4
    spread = jnp.where(own_lanes, spread, 0.0)
    folded = spread[:, 0:128] + spread[:, 128:256]
    folded = folded + pltpu.roll(folded, 64, 1)
    query_rows[...] = folded
    wide = jnp.concatenate([folded] * 4, axis=1)
    block = iota((256, 512), 1) // HEAD_DIM == (iota((256, 512), 0) // 4) % 8
    left[...] = jnp.where(block, wide, 0.0).astype(BF)

    lane = iota((64, 128), 1)
    sums = []
    for g in range(8):
        rows = slice(32 * g, 32 * g + 32)
        scores = dot(left[rows, :], keys[512 * g : 512 * g + 512, :]) * (HEAD_DIM ** (-0.5))
        scores = scores + decay[8 * g : 8 * g + 8].reshape(32, 1024)
        peak = jnp.max(scores, axis=1, keepdims=True)
        weights = jnp.exp(scores - peak)
        mass = jnp.sum(weights, axis=1, keepdims=True)
        peaks[rows, :] = jnp.broadcast_to(peak, (32, 128))
        masses[rows, :] = jnp.broadcast_to(mass, (32, 128))
        weights = weights.astype(BF)
        summed = dot_t(values[512 * g : 512 * g + 512, :], jnp.concatenate([weights] * 4, axis=0))
        total = jnp.zeros((64, 128), F32) if g % 4 == 0 else sums.pop()
        for k in range(8):
            own = lane // 4 == 8 * (g % 4) + k
            total = jnp.where(own, summed[64 * k : 64 * k + 64], total)
        sums.append(total)

    me = lax.axis_index("kv")
    tile = me // 2
    own_scale = scales[pl.ds(pl.multiple_of(8 * tile, 8), 8), :]
    key_value = (own_scale * extra[:, 0:128]).astype(BF)
    forget = extra[:, 128:256]
    forget = own_scale * (forget + pltpu.roll(forget, 124, 1))
    log_forget = -(jnp.maximum(-forget, 0.0) + jnp.log1p(jnp.exp(-jnp.abs(forget))))
    log_forget = jnp.where(iota((8, 128), 1) < 4, log_forget, 0.0)
    repeat8 = iota((128, 8), 0) // 4 % 8 == iota((128, 8), 1)
    key_value = dot(repeat8.astype(BF), key_value)
    log_forget = jnp.dot(
        repeat8[0:32].astype(F32), log_forget, preferred_element_type=F32, precision=lax.Precision.HIGHEST
    )
    mine = iota((32, 128), 1) == iota((32, 128), 0) % 4
    log_forget = jnp.sum(jnp.where(mine, log_forget, 0.0), axis=1, keepdims=True)
    at = pl.ds(pl.multiple_of(32 * tile, 32), 32)
    lower = iota((32, 128), 1) < 64
    own = jnp.sum(jnp.where(lower, query_rows[at, :] * key_value[0:32], 0.0), axis=1, keepdims=True)
    own = own * (HEAD_DIM ** (-0.5)) - log_forget
    own = jnp.concatenate([own] * 4, axis=0)
    place = iota((128, 128), 0) == iota((128, 128), 1)
    own = jnp.sum(jnp.where(place, own, 0.0), axis=0, keepdims=True)
    pick = (iota((64, 128), 1) == iota((64, 128), 0) + 64).astype(BF)
    value = dot_t(pick, key_value.astype(BF))

    line = iota((8, 128), 0)
    slot = iota((1, 128), 1) // 32
    packed = jnp.zeros((8, 128), F32)
    for j in range(2):
        rows = slice(128 * j, 128 * j + 128)
        peak = jnp.sum(jnp.where(place, peaks[rows, :], 0.0), axis=0, keepdims=True)
        mass = jnp.sum(jnp.where(place, masses[rows, :], 0.0), axis=0, keepdims=True)
        here = (slot + 4 * j == tile) & (me % 2 == 0)
        joined = jnp.where(here, own, peak - 1e30)
        top = jnp.maximum(peak, joined)
        keep = jnp.exp(peak - top)
        weight = jnp.exp(joined - top)
        mass = mass * keep + weight
        out[64 * j : 64 * j + 64, :] = ((sums[j] * keep + high(weight) * value) / mass).astype(BF)
        level = top + jnp.log(mass)
        for k in range(3):
            piece = high(level)
            packed = jnp.where(line == 3 * j + k, piece, packed)
            level = level - piece
    out[128:136, :] = packed.astype(BF)


def merge_kernel(parts, w_out, out):
    extra = parts[:, 128:136, :].astype(F32)
    row, column = iota((128, 128), 0), iota((128, 128), 1)
    order = ((row % 32 == column // 4) & (row // 32 == column % 4)).astype(BF)
    heads = []
    for j in range(2):
        level = extra[:, 3 * j, :] + extra[:, 3 * j + 1, :] + extra[:, 3 * j + 2, :]
        factor = jnp.exp(level - jnp.max(level, axis=0, keepdims=True))
        factor = factor / jnp.sum(factor, axis=0, keepdims=True)
        total = jnp.zeros((64, 128), F32)
        for i in range(16):
            total = total + parts[i, 64 * j : 64 * j + 64, :].astype(F32) * factor[i : i + 1, :]
        heads.append(dot_t(order, total.astype(BF)).astype(BF))
    partial = jnp.zeros((64, 256), F32)
    for h in range(4):
        attended = jnp.concatenate([heads[0][32 * h : 32 * h + 32], heads[1][32 * h : 32 * h + 32]], axis=0)
        partial = partial + dot(attended, w_out[64 * h : 64 * h + 64, :])
    partial = partial.astype(BF)
    for i in range(8):
        out[i] = partial


def up_kernel(parts, tokens, gain, w_up, residual_out, out):
    attn = parts[0].astype(F32)
    for i in range(1, 8):
        attn = attn + parts[i].astype(F32)
    residual = (tokens[...].astype(F32) + high(attn)).astype(BF)
    residual_out[...] = residual
    wide = residual.astype(F32)
    squares = jnp.sum(wide * wide, axis=1, keepdims=True)
    squares_high = high(squares)
    row_high = column_to_row(squares_high, 128, 0)
    row_low = column_to_row(squares - squares_high, 128, 0)
    line = iota((8, 128), 0)
    tile = jnp.where(line == 0, row_high, jnp.where(line == 1, row_low, 0.0)).astype(BF)
    normed = (wide * gain[...]).astype(BF)
    for p in range(0, 16, 2):
        up = dot(normed, w_up[:, 128 * p : 128 * p + 256]).astype(BF)
        for k in range(2):
            out[p + k, 0:64, :] = up[:, 128 * k : 128 * k + 128]
            out[p + k, 64:72, :] = tile


def hidden_kernel(parts, out):
    up = parts[0, 0:64, :].astype(F32)
    extra = parts[0, 64:72, :].astype(F32)
    for i in range(1, 16):
        up = up + parts[i, 0:64, :].astype(F32)
        extra = extra + parts[i, 64:72, :].astype(F32)
    squares = row_to_column(extra[0:1] + extra[1:2], 64, 0)
    up = lax.rsqrt(squares / D + EPS) * up
    up = jnp.maximum(up, 0.0)
    hidden = (up * up).astype(BF)
    for i in range(16):
        out[i] = hidden


def down_kernel(parts, w_down, out):
    down = jnp.zeros((64, 256), F32)
    for i in range(0, 16, 2):
        pair = jnp.concatenate([parts[i], parts[i + 1]], axis=1)
        down = down + dot(pair, w_down[128 * i : 128 * i + 256, :])
    down = down.astype(BF)
    for i in range(8):
        out[i] = down


def finish_kernel(parts, residual, out):
    down = parts[0].astype(F32)
    for i in range(1, 8):
        down = down + parts[i].astype(F32)
    out[...] = (residual[...].astype(F32) + high(down)).astype(BF)


def exchange(array, axis):
    return lax.all_to_all(array, axis, split_axis=0, concat_axis=0, tiled=True)


def sent(array, axis):
    return exchange(jnp.broadcast_to(array, (lax.axis_size(axis), *array.shape)), axis)


def shards(
    tokens, mix_gain, w_query, w_key, w_value, w_forget, query_gain,
    key_cache, value_cache, decay_cache, w_out, mlp_gain, w_up, w_down,
):
    shape = jax.ShapeDtypeStruct
    head = call(head_kernel, shape((8, 128), F32), "head", cost=3 * 10**9)()
    operands = (tokens, mix_gain.reshape(1, -1), w_query, w_key.T, w_value.T, w_forget.T)
    query, extra = call(project_kernel, (shape((64, 256), BF), shape((64, 256), BF)), "project")(head, *operands)
    message = call(spread_kernel, shape((16, 72, 256), BF), "spread", cost=10**10)(query, extra)
    message = exchange(message, "kv")
    part = call(
        attend_kernel,
        shape((136, 128), BF),
        "attend",
        scratch=[
            pltpu.VMEM((64, 128), F32),
            pltpu.VMEM((256, 128), F32),
            pltpu.VMEM((256, 512), BF),
            pltpu.VMEM((256, 128), F32),
            pltpu.VMEM((256, 128), F32),
        ],

        limit=8 << 20,
    )(
        message,
        query_gain.reshape(1, -1),
        key_cache.reshape(4096, 1024),
        value_cache.reshape(4096, 1024),
        decay_cache,
    )
    message = call(merge_kernel, shape((8, 64, 256), BF), "merge")(sent(part, "kv"), w_out)
    residual, message = call(up_kernel, (shape((64, 256), BF), shape((16, 72, 128), BF)), "up")(
        exchange(message, "tp"), tokens, mlp_gain.reshape(1, -1), w_up
    )
    message = call(hidden_kernel, shape((16, 64, 128), BF), "hidden")(exchange(message, "kv"))
    message = call(down_kernel, shape((8, 64, 256), BF), "down")(exchange(message, "kv"), w_down)
    return call(finish_kernel, shape((64, 256), BF), "finish")(exchange(message, "tp"), residual)


def solution(mesh):
    return jax.shard_map(
        shards,
        mesh=mesh,
        in_specs=(
            P(None, "kv"),
            P("kv"),
            P("kv", "tp"),
            P("kv", "tp"),
            P("kv", "tp"),
            P("kv", "tp"),
            P(),
            P(None, "tp", None, "kv"),
            P(None, "tp", None, "kv"),
            P(None, "tp", "kv"),
            P("tp", "kv"),
            P("kv"),
            P("kv", "tp"),
            P("tp", "kv"),
        ),
        out_specs=P(None, "kv"),
        check_vma=False,
    )
```

```python
import jax
import jax.numpy as jnp
from jax import lax
from jax.experimental import pallas as pl
from jax.experimental.pallas import tpu as pltpu
from jax.sharding import PartitionSpec as P

D = 4096
HEAD_DIM = 64
EPS = 1e-06
BF = jnp.bfloat16
F32 = jnp.float32

VM = pl.BlockSpec(memory_space=pltpu.VMEM)


def iota(shape, dim):
    return lax.broadcasted_iota(jnp.int32, shape, dim)


def dot(a, b):
    return jnp.dot(a, b, preferred_element_type=F32)


def dot_t(a, b):
    return lax.dot_general(a, b, (((1,), (1,)), ((), ())), preferred_element_type=F32)


def high(a):
    return a.astype(BF).astype(F32)


def column_to_row(column, width, at):
    n = column.shape[0]
    place = iota((n, width), 1) == iota((n, width), 0) + at
    return jnp.sum(jnp.where(place, column, 0.0), axis=0, keepdims=True)


def row_to_column(row, n, at):
    width = row.shape[1]
    place = iota((n, width), 1) == iota((n, width), 0) + at
    return jnp.sum(jnp.where(place, row, 0.0), axis=1, keepdims=True)


def call(kernel, outs, name, scratch=(), in_specs=None, limit=16 << 20, cost=None):
    def run(*args):
        return pl.pallas_call(
            kernel,
            out_shape=outs,
            in_specs=in_specs or [VM] * len(args),
            out_specs=jax.tree.map(lambda _: VM, outs),
            scratch_shapes=list(scratch),
            compiler_params=pltpu.CompilerParams(vmem_limit_bytes=limit),
            name=name,
            cost_estimate=cost and pl.CostEstimate(flops=cost, bytes_accessed=cost // 100, transcendentals=0),
        )(*args)

    return run


def project_kernel(head, tokens, gain, w_query, w_key, w_value, w_forget, query_out, extra_out):
    stream = tokens[...].astype(F32)
    squares = jnp.sum(stream * stream, axis=1, keepdims=True)
    normed = (stream * gain[...]).astype(BF)
    query_out[...] = dot(normed, w_query[...]).astype(BF)
    key_value = dot_t(normed, jnp.concatenate([w_key[...], w_value[...]], axis=0))
    forget_w = w_forget[...].astype(F32)
    forget_w = jnp.concatenate([forget_w, forget_w, jnp.zeros((120, 256), F32)], axis=0)
    forget = dot_t(normed, forget_w.astype(BF))
    forget = jnp.where(iota(forget.shape, 1) < 4, high(forget), forget - high(forget))
    squares_high = high(squares)
    row_high = column_to_row(squares_high, 128, 64)
    row_low = column_to_row(squares - squares_high, 128, 64)
    line = iota((64, 128), 0) % 8
    forget = forget + jnp.where(line == 0, row_high, jnp.where(line == 1, row_low, 0.0))
    extra_out[:, 0:128] = key_value.astype(BF)
    extra_out[:, 128:256] = forget.astype(BF)


def head_kernel(out):
    out[...] = jnp.zeros_like(out)


def spread_kernel(query, extra, out):
    for p in range(16):
        out[p, 0:64, :] = query[...]
        out[p, 64:72, :] = extra[8 * (p // 2) : 8 * (p // 2) + 8, :]


def attend_kernel(
    parts, query_gain, keys, values, decay, out,
    scales, query_rows, left, peaks, masses,
):
    extra = [parts[i, 64:72, :].astype(F32) for i in range(16)]
    raw = [parts[i, 0:64, :].astype(F32) for i in range(16)]
    while len(raw) > 1:
        raw = [a + b for a, b in zip(raw[::2], raw[1::2])]
        extra = [a + b for a, b in zip(extra[::2], extra[1::2])]
    raw, extra = raw[0], extra[0]
    squares = row_to_column(extra[0:1, 128:256] + extra[1:2, 128:256], 64, 64)
    scale = lax.rsqrt(squares / D + EPS)
    scales[...] = jnp.broadcast_to(scale, (64, 128))
    head_of = iota((64, 256), 1) // HEAD_DIM
    power = raw * raw
    inverse = jnp.zeros((64, 256), F32)
    for h in range(4):
        mean = jnp.sum(jnp.where(head_of == h, power, 0.0), axis=1, keepdims=True) / HEAD_DIM
        inverse = jnp.where(head_of == h, scale * lax.rsqrt(scale * scale * mean + EPS), inverse)
    gain = query_gain[...]
    gain = jnp.concatenate([gain, gain, gain, gain], axis=1)
    query = (raw * inverse * gain).astype(BF)

    repeat = (iota((256, 64), 0) // 4 == iota((256, 64), 1)).astype(BF)
    spread = dot(repeat, query)
    own_lanes = iota((256, 256), 1) // HEAD_DIM == iota((256, 256), 0) % 4
    spread = jnp.where(own_lanes, spread, 0.0)
    folded = spread[:, 0:128] + spread[:, 128:256]
    folded = folded + pltpu.roll(folded, 64, 1)
    query_rows[...] = folded
    wide = jnp.concatenate([folded] * 2, axis=1)
    block = iota((256, 256), 1) // HEAD_DIM == (iota((256, 256), 0) // 4) % 4
    left[...] = jnp.where(block, wide * (HEAD_DIM ** (-0.5)), 0.0).astype(BF)

    me = lax.axis_index("kv")
    tile = me // 2
    own_scale = scales[pl.ds(pl.multiple_of(8 * tile, 8), 8), :]
    key_value = (own_scale * extra[:, 0:128]).astype(BF)
    forget = extra[:, 128:256]
    forget = own_scale * (forget + pltpu.roll(forget, 124, 1))
    log_forget = -(jnp.maximum(-forget, 0.0) + jnp.log1p(jnp.exp(-jnp.abs(forget))))
    log_forget = jnp.where(iota((8, 128), 1) < 4, log_forget, 0.0)
    repeat8 = iota((128, 8), 0) // 4 % 8 == iota((128, 8), 1)
    key_value = dot(repeat8.astype(BF), key_value)
    log_forget = jnp.dot(
        repeat8[0:32].astype(F32), log_forget, preferred_element_type=F32, precision=lax.Precision.HIGHEST
    )
    mine = iota((32, 128), 1) == iota((32, 128), 0) % 4
    log_forget = jnp.sum(jnp.where(mine, log_forget, 0.0), axis=1, keepdims=True)
    at = pl.ds(pl.multiple_of(32 * tile, 32), 32)
    lower = iota((32, 128), 1) < 64
    own = jnp.sum(jnp.where(lower, query_rows[at, :] * key_value[0:32], 0.0), axis=1, keepdims=True)
    own = own * (HEAD_DIM ** (-0.5)) - log_forget
    own = jnp.concatenate([own] * 4, axis=0)
    place = iota((128, 128), 0) == iota((128, 128), 1)
    own = jnp.sum(jnp.where(place, own, 0.0), axis=0, keepdims=True)
    pick = (iota((64, 128), 1) == iota((64, 128), 0) + 64).astype(BF)
    value = dot_t(pick, key_value.astype(BF))

    lane = iota((64, 16), 1)
    folds = []
    def score(g):
        scores = dot(left[16 * g : 16 * g + 16, :], keys[256 * g : 256 * g + 256, :])
        return scores + decay[4 * g : 4 * g + 4].reshape(16, 1024)

    ahead = [score(g) for g in range(8)]
    for g in range(16):
        rows = slice(16 * g, 16 * g + 16)
        scores = ahead.pop(0)
        peak = jnp.max(scores, axis=1, keepdims=True)
        weights = jnp.exp(scores - peak)
        mass = jnp.sum(weights, axis=1, keepdims=True)
        peaks[rows, :] = jnp.broadcast_to(peak, (16, 128))
        masses[rows, :] = jnp.broadcast_to(mass, (16, 128))
        weights = weights.astype(BF)
        if g + 8 < 16:
            ahead.append(score(g + 8))
        summed = dot_t(values[256 * g : 256 * g + 256, :], weights)
        total = summed[0:64]
        for k in range(1, 4):
            total = jnp.where(lane // 4 == k, summed[64 * k : 64 * k + 64], total)
        folds.append(total)
    sums = [jnp.concatenate(folds[8 * j : 8 * j + 8], axis=1) for j in range(2)]

    line = iota((8, 128), 0)
    slot = iota((1, 128), 1) // 32
    packed = jnp.zeros((8, 128), F32)
    for j in range(2):
        rows = slice(128 * j, 128 * j + 128)
        peak = jnp.sum(jnp.where(place, peaks[rows, :], 0.0), axis=0, keepdims=True)
        mass = jnp.sum(jnp.where(place, masses[rows, :], 0.0), axis=0, keepdims=True)
        here = (slot + 4 * j == tile) & (me % 2 == 0)
        joined = jnp.where(here, own, peak - 1e30)
        top = jnp.maximum(peak, joined)
        keep = jnp.exp(peak - top)
        weight = jnp.exp(joined - top)
        mass = mass * keep + weight
        out[64 * j : 64 * j + 64, :] = ((sums[j] * keep + high(weight) * value) / mass).astype(BF)
        level = top + jnp.log(mass)
        for k in range(3):
            piece = high(level)
            packed = jnp.where(line == 3 * j + k, piece, packed)
            level = level - piece
    out[128:136, :] = packed.astype(BF)


def merge_kernel(parts, w_out, out):
    extra = parts[:, 128:136, :].astype(F32)
    row, column = iota((128, 128), 0), iota((128, 128), 1)
    order = ((row % 32 == column // 4) & (row // 32 == column % 4)).astype(BF)
    heads = []
    for j in range(2):
        level = extra[:, 3 * j, :] + extra[:, 3 * j + 1, :] + extra[:, 3 * j + 2, :]
        factor = jnp.exp(level - jnp.max(level, axis=0, keepdims=True))
        factor = factor / jnp.sum(factor, axis=0, keepdims=True)
        total = jnp.zeros((64, 128), F32)
        for i in range(16):
            total = total + parts[i, 64 * j : 64 * j + 64, :].astype(F32) * factor[i : i + 1, :]
        heads.append(dot_t(order, total.astype(BF)).astype(BF))
    partial = jnp.zeros((64, 256), F32)
    for h in range(4):
        attended = jnp.concatenate([heads[0][32 * h : 32 * h + 32], heads[1][32 * h : 32 * h + 32]], axis=0)
        partial = partial + dot(attended, w_out[64 * h : 64 * h + 64, :])
    partial = partial.astype(BF)
    for i in range(8):
        out[i] = partial


def up_kernel(parts, tokens, gain, w_up, residual_out, out):
    attn = parts[0].astype(F32)
    for i in range(1, 8):
        attn = attn + parts[i].astype(F32)
    residual = (tokens[...].astype(F32) + high(attn)).astype(BF)
    residual_out[...] = residual
    wide = residual.astype(F32)
    squares = jnp.sum(wide * wide, axis=1, keepdims=True)
    squares_high = high(squares)
    row_high = column_to_row(squares_high, 128, 0)
    row_low = column_to_row(squares - squares_high, 128, 0)
    line = iota((8, 128), 0)
    tile = jnp.where(line == 0, row_high, jnp.where(line == 1, row_low, 0.0)).astype(BF)
    normed = (wide * gain[...]).astype(BF)
    for p in range(0, 16, 2):
        up = dot(normed, w_up[:, 128 * p : 128 * p + 256]).astype(BF)
        for k in range(2):
            out[p + k, 0:64, :] = up[:, 128 * k : 128 * k + 128]
            out[p + k, 64:72, :] = tile


def hidden_kernel(parts, out):
    up = parts[0, 0:64, :].astype(F32)
    extra = parts[0, 64:72, :].astype(F32)
    for i in range(1, 16):
        up = up + parts[i, 0:64, :].astype(F32)
        extra = extra + parts[i, 64:72, :].astype(F32)
    squares = row_to_column(extra[0:1] + extra[1:2], 64, 0)
    up = lax.rsqrt(squares / D + EPS) * up
    up = jnp.maximum(up, 0.0)
    hidden = (up * up).astype(BF)
    for i in range(16):
        out[i] = hidden


def down_kernel(parts, w_down, out):
    down = jnp.zeros((64, 256), F32)
    for i in range(0, 16, 2):
        pair = jnp.concatenate([parts[i], parts[i + 1]], axis=1)
        down = down + dot(pair, w_down[128 * i : 128 * i + 256, :])
    down = down.astype(BF)
    for i in range(8):
        out[i] = down


def finish_kernel(parts, residual, out):
    down = parts[0].astype(F32)
    for i in range(1, 8):
        down = down + parts[i].astype(F32)
    out[...] = (residual[...].astype(F32) + high(down)).astype(BF)


def exchange(array, axis):
    return lax.all_to_all(array, axis, split_axis=0, concat_axis=0, tiled=True)


def sent(array, axis):
    return exchange(jnp.broadcast_to(array, (lax.axis_size(axis), *array.shape)), axis)


def attend(message, query_gain, key_cache, value_cache, decay_cache):
    return call(
        attend_kernel,
        jax.ShapeDtypeStruct((136, 128), BF),
        "attend",
        scratch=[
            pltpu.VMEM((64, 128), F32),
            pltpu.VMEM((256, 128), F32),
            pltpu.VMEM((256, 256), BF),
            pltpu.VMEM((256, 128), F32),
            pltpu.VMEM((256, 128), F32),
        ],
        limit=8 << 20,
    )(
        message,
        query_gain.reshape(1, -1),
        key_cache.reshape(4096, 1024),
        value_cache.reshape(4096, 1024),
        decay_cache,
    )


def shards(
    tokens, mix_gain, w_query, w_key, w_value, w_forget, query_gain,
    key_cache, value_cache, decay_cache, w_out, mlp_gain, w_up, w_down,
):
    shape = jax.ShapeDtypeStruct
    head = call(head_kernel, shape((8, 128), F32), "head", cost=3 * 10**9)()
    operands = (tokens, mix_gain.reshape(1, -1), w_query, w_key.T, w_value.T, w_forget.T)
    query, extra = call(project_kernel, (shape((64, 256), BF), shape((64, 256), BF)), "project")(head, *operands)
    message = call(spread_kernel, shape((16, 72, 256), BF), "spread", cost=10**10)(query, extra)
    message = exchange(message, "kv")
    part = attend(message, query_gain, key_cache, value_cache, decay_cache)
    message = call(merge_kernel, shape((8, 64, 256), BF), "merge")(sent(part, "kv"), w_out)
    residual, message = call(up_kernel, (shape((64, 256), BF), shape((16, 72, 128), BF)), "up")(
        exchange(message, "tp"), tokens, mlp_gain.reshape(1, -1), w_up
    )
    message = call(hidden_kernel, shape((16, 64, 128), BF), "hidden")(exchange(message, "kv"))
    message = call(down_kernel, shape((8, 64, 256), BF), "down")(exchange(message, "kv"), w_down)
    return call(finish_kernel, shape((64, 256), BF), "finish")(exchange(message, "tp"), residual)


def solution(mesh):
    return jax.shard_map(
        shards,
        mesh=mesh,
        in_specs=(
            P(None, "kv"),
            P("kv"),
            P("kv", "tp"),
            P("kv", "tp"),
            P("kv", "tp"),
            P("kv", "tp"),
            P(),
            P(None, "tp", None, "kv"),
            P(None, "tp", None, "kv"),
            P(None, "tp", "kv"),
            P("tp", "kv"),
            P("kv"),
            P("kv", "tp"),
            P("tp", "kv"),
        ),
        out_specs=P(None, "kv"),
        check_vma=False,
    )
```

```python
import jax
import jax.numpy as jnp
from jax import lax
from jax.experimental import pallas as pl
from jax.experimental.pallas import tpu as pltpu
from jax.sharding import Mesh
from jax.sharding import PartitionSpec as P

D = 4096
HEAD_DIM = 64
EPS = 1e-06
TP = ("x", "core")
BF = jnp.bfloat16
F32 = jnp.float32

VM = pl.BlockSpec(memory_space=pltpu.VMEM)


def iota(shape, dim):
    return lax.broadcasted_iota(jnp.int32, shape, dim)


def dot(a, b):
    return jnp.dot(a, b, preferred_element_type=F32)


def dot_t(a, b):
    return lax.dot_general(a, b, (((1,), (1,)), ((), ())), preferred_element_type=F32)


def high(a):
    return a.astype(BF).astype(F32)


def column_to_row(column, width, at):
    n = column.shape[0]
    place = iota((n, width), 1) == iota((n, width), 0) + at
    return jnp.sum(jnp.where(place, column, 0.0), axis=0, keepdims=True)


def row_to_column(row, n, at):
    width = row.shape[1]
    place = iota((n, width), 1) == iota((n, width), 0) + at
    return jnp.sum(jnp.where(place, row, 0.0), axis=1, keepdims=True)


def call(kernel, outs, name, scratch=(), in_specs=None, limit=16 << 20, cost=None):
    def run(*args):
        return pl.pallas_call(
            kernel,
            out_shape=outs,
            in_specs=in_specs or [VM] * len(args),
            out_specs=jax.tree.map(lambda _: VM, outs),
            scratch_shapes=list(scratch),
            compiler_params=pltpu.CompilerParams(vmem_limit_bytes=limit),
            name=name,
            cost_estimate=cost and pl.CostEstimate(flops=cost, bytes_accessed=cost // 100, transcendentals=0),
        )(*args)

    return run


def project_kernel(head, tokens, gain, w_query, w_key, w_value, w_forget, query_out, extra_out):
    stream = tokens[...].astype(F32)
    squares = jnp.sum(stream * stream, axis=1, keepdims=True)
    normed = (stream * gain[...]).astype(BF)
    query_out[...] = dot(normed, w_query[...]).astype(BF)
    key_value = dot_t(normed, jnp.concatenate([w_key[...], w_value[...]], axis=0))
    forget_w = w_forget[...].astype(F32)
    forget_w = jnp.concatenate([forget_w, forget_w, jnp.zeros((120, 256), F32)], axis=0)
    forget = dot_t(normed, forget_w.astype(BF))
    forget = jnp.where(iota(forget.shape, 1) < 4, high(forget), forget - high(forget))
    squares_high = high(squares)
    row_high = column_to_row(squares_high, 128, 64)
    row_low = column_to_row(squares - squares_high, 128, 64)
    line = iota((64, 128), 0) % 8
    forget = forget + jnp.where(line == 0, row_high, jnp.where(line == 1, row_low, 0.0))
    extra_out[:, 0:128] = key_value.astype(BF)
    extra_out[:, 128:256] = forget.astype(BF)


def head_kernel(out):
    out[...] = jnp.zeros_like(out)


def spread_kernel(query, extra, out):
    for p in range(16):
        out[p, 0:64, :] = query[...]
        out[p, 64:72, :] = extra[8 * (p // 2) : 8 * (p // 2) + 8, :]


def attend_kernel(
    parts, query_gain, keys, values, decay, out,
    scales, query_rows, left, peaks, masses,
):
    extra = [parts[i, 64:72, :].astype(F32) for i in range(16)]
    raw = [parts[i, 0:64, :].astype(F32) for i in range(16)]
    while len(raw) > 1:
        raw = [a + b for a, b in zip(raw[::2], raw[1::2])]
        extra = [a + b for a, b in zip(extra[::2], extra[1::2])]
    raw, extra = raw[0], extra[0]
    squares = row_to_column(extra[0:1, 128:256] + extra[1:2, 128:256], 64, 64)
    scale = lax.rsqrt(squares / D + EPS)
    scales[...] = jnp.broadcast_to(scale, (64, 128))
    head_of = iota((64, 256), 1) // HEAD_DIM
    power = raw * raw
    inverse = jnp.zeros((64, 256), F32)
    for h in range(4):
        mean = jnp.sum(jnp.where(head_of == h, power, 0.0), axis=1, keepdims=True) / HEAD_DIM
        inverse = jnp.where(head_of == h, scale * lax.rsqrt(scale * scale * mean + EPS), inverse)
    gain = query_gain[...]
    gain = jnp.concatenate([gain, gain, gain, gain], axis=1)
    query = (raw * inverse * gain).astype(BF)

    repeat = (iota((256, 64), 0) // 4 == iota((256, 64), 1)).astype(BF)
    spread = dot(repeat, query)
    own_lanes = iota((256, 256), 1) // HEAD_DIM == iota((256, 256), 0) % 4
    spread = jnp.where(own_lanes, spread, 0.0)
    folded = spread[:, 0:128] + spread[:, 128:256]
    folded = folded + pltpu.roll(folded, 64, 1)
    query_rows[...] = folded
    wide = jnp.concatenate([folded] * 2, axis=1)
    block = iota((256, 256), 1) // HEAD_DIM == (iota((256, 256), 0) // 4) % 4
    left[...] = jnp.where(block, wide * (HEAD_DIM ** (-0.5)), 0.0).astype(BF)

    me = lax.axis_index("kv")
    tile = me // 2
    own_scale = scales[pl.ds(pl.multiple_of(8 * tile, 8), 8), :]
    key_value = (own_scale * extra[:, 0:128]).astype(BF)
    forget = extra[:, 128:256]
    forget = own_scale * (forget + pltpu.roll(forget, 124, 1))
    log_forget = -(jnp.maximum(-forget, 0.0) + jnp.log1p(jnp.exp(-jnp.abs(forget))))
    log_forget = jnp.where(iota((8, 128), 1) < 4, log_forget, 0.0)
    repeat8 = iota((128, 8), 0) // 4 % 8 == iota((128, 8), 1)
    key_value = dot(repeat8.astype(BF), key_value)
    log_forget = jnp.dot(
        repeat8[0:32].astype(F32), log_forget, preferred_element_type=F32, precision=lax.Precision.HIGHEST
    )
    mine = iota((32, 128), 1) == iota((32, 128), 0) % 4
    log_forget = jnp.sum(jnp.where(mine, log_forget, 0.0), axis=1, keepdims=True)
    at = pl.ds(pl.multiple_of(32 * tile, 32), 32)
    lower = iota((32, 128), 1) < 64
    own = jnp.sum(jnp.where(lower, query_rows[at, :] * key_value[0:32], 0.0), axis=1, keepdims=True)
    own = own * (HEAD_DIM ** (-0.5)) - log_forget
    own = jnp.concatenate([own] * 4, axis=0)
    place = iota((128, 128), 0) == iota((128, 128), 1)
    own = jnp.sum(jnp.where(place, own, 0.0), axis=0, keepdims=True)
    pick = (iota((64, 128), 1) == iota((64, 128), 0) + 64).astype(BF)
    value = dot_t(pick, key_value.astype(BF))

    lane = iota((64, 16), 1)
    folds = []
    def score(g):
        scores = dot(left[16 * g : 16 * g + 16, :], keys[256 * g : 256 * g + 256, :])
        return scores + decay[4 * g : 4 * g + 4].reshape(16, 1024)

    ahead = [score(g) for g in range(8)]
    for g in range(16):
        rows = slice(16 * g, 16 * g + 16)
        scores = ahead.pop(0)
        peak = jnp.max(scores, axis=1, keepdims=True)
        weights = jnp.exp(scores - peak)
        mass = jnp.sum(weights, axis=1, keepdims=True)
        peaks[rows, :] = jnp.broadcast_to(peak, (16, 128))
        masses[rows, :] = jnp.broadcast_to(mass, (16, 128))
        weights = weights.astype(BF)
        if g + 8 < 16:
            ahead.append(score(g + 8))
        summed = dot_t(values[256 * g : 256 * g + 256, :], weights)
        total = summed[0:64]
        for k in range(1, 4):
            total = jnp.where(lane // 4 == k, summed[64 * k : 64 * k + 64], total)
        folds.append(total)
    sums = [jnp.concatenate(folds[8 * j : 8 * j + 8], axis=1) for j in range(2)]

    line = iota((8, 128), 0)
    slot = iota((1, 128), 1) // 32
    packed = jnp.zeros((8, 128), F32)
    for j in range(2):
        rows = slice(128 * j, 128 * j + 128)
        peak = jnp.sum(jnp.where(place, peaks[rows, :], 0.0), axis=0, keepdims=True)
        mass = jnp.sum(jnp.where(place, masses[rows, :], 0.0), axis=0, keepdims=True)
        here = (slot + 4 * j == tile) & (me % 2 == 0)
        joined = jnp.where(here, own, peak - 1e30)
        top = jnp.maximum(peak, joined)
        keep = jnp.exp(peak - top)
        weight = jnp.exp(joined - top)
        mass = mass * keep + weight
        out[64 * j : 64 * j + 64, :] = ((sums[j] * keep + high(weight) * value) / mass).astype(BF)
        level = top + jnp.log(mass)
        for k in range(3):
            piece = high(level)
            packed = jnp.where(line == 3 * j + k, piece, packed)
            level = level - piece
    out[128:136, :] = packed.astype(BF)


def merge_kernel(parts, w_out, out):
    extra = parts[:, 128:136, :].astype(F32)
    row, column = iota((128, 128), 0), iota((128, 128), 1)
    order = ((row % 32 == column // 4) & (row // 32 == column % 4)).astype(BF)
    heads = []
    for j in range(2):
        level = extra[:, 3 * j, :] + extra[:, 3 * j + 1, :] + extra[:, 3 * j + 2, :]
        factor = jnp.exp(level - jnp.max(level, axis=0, keepdims=True))
        factor = factor / jnp.sum(factor, axis=0, keepdims=True)
        total = jnp.zeros((64, 128), F32)
        for i in range(16):
            total = total + parts[i, 64 * j : 64 * j + 64, :].astype(F32) * factor[i : i + 1, :]
        heads.append(dot_t(order, total.astype(BF)).astype(BF))
    partial = jnp.zeros((64, 256), F32)
    for h in range(4):
        attended = jnp.concatenate([heads[0][32 * h : 32 * h + 32], heads[1][32 * h : 32 * h + 32]], axis=0)
        partial = partial + dot(attended, w_out[64 * h : 64 * h + 64, :])
    out[...] = partial.astype(BF)


def pair_kernel(mine, partner, out):
    total = (mine[...].astype(F32) + partner[...].astype(F32)).astype(BF)
    for i in range(4):
        out[i] = total


def up_kernel(parts, tokens, gain, w_up, residual_out, out):
    attn = parts[0].astype(F32)
    for i in range(1, 4):
        attn = attn + parts[i].astype(F32)
    residual = (tokens[...].astype(F32) + high(attn)).astype(BF)
    residual_out[...] = residual
    wide = residual.astype(F32)
    squares = jnp.sum(wide * wide, axis=1, keepdims=True)
    squares_high = high(squares)
    row_high = column_to_row(squares_high, 128, 0)
    row_low = column_to_row(squares - squares_high, 128, 0)
    line = iota((8, 128), 0)
    tile = jnp.where(line == 0, row_high, jnp.where(line == 1, row_low, 0.0)).astype(BF)
    normed = (wide * gain[...]).astype(BF)
    for p in range(0, 16, 2):
        up = dot(normed, w_up[:, 128 * p : 128 * p + 256]).astype(BF)
        for k in range(2):
            out[p + k, 0:64, :] = up[:, 128 * k : 128 * k + 128]
            out[p + k, 64:72, :] = tile


def hidden_kernel(parts, out):
    up = parts[0, 0:64, :].astype(F32)
    extra = parts[0, 64:72, :].astype(F32)
    for i in range(1, 16):
        up = up + parts[i, 0:64, :].astype(F32)
        extra = extra + parts[i, 64:72, :].astype(F32)
    squares = row_to_column(extra[0:1] + extra[1:2], 64, 0)
    up = lax.rsqrt(squares / D + EPS) * up
    up = jnp.maximum(up, 0.0)
    hidden = (up * up).astype(BF)
    for i in range(16):
        out[i] = hidden


def down_kernel(parts, w_down, out):
    down = jnp.zeros((64, 256), F32)
    for i in range(0, 16, 2):
        pair = jnp.concatenate([parts[i], parts[i + 1]], axis=1)
        down = down + dot(pair, w_down[128 * i : 128 * i + 256, :])
    out[...] = down.astype(BF)


def finish_kernel(parts, residual, out):
    down = parts[0].astype(F32)
    for i in range(1, 4):
        down = down + parts[i].astype(F32)
    out[...] = (residual[...].astype(F32) + high(down)).astype(BF)


def exchange(array, axis):
    return lax.all_to_all(array, axis, split_axis=0, concat_axis=0, tiled=True)


def pair_sum(partial):
    partner = lax.ppermute(partial, "core", [(0, 1), (1, 0)])
    message = call(pair_kernel, jax.ShapeDtypeStruct((4, 64, 256), BF), "pair")(partial, partner)
    return exchange(message, "x")


def sent(array, axis):
    return exchange(jnp.broadcast_to(array, (lax.axis_size(axis), *array.shape)), axis)


def attend(message, query_gain, key_cache, value_cache, decay_cache):
    return call(
        attend_kernel,
        jax.ShapeDtypeStruct((136, 128), BF),
        "attend",
        scratch=[
            pltpu.VMEM((64, 128), F32),
            pltpu.VMEM((256, 128), F32),
            pltpu.VMEM((256, 256), BF),
            pltpu.VMEM((256, 128), F32),
            pltpu.VMEM((256, 128), F32),
        ],
        limit=8 << 20,
    )(
        message,
        query_gain.reshape(1, -1),
        key_cache.reshape(4096, 1024),
        value_cache.reshape(4096, 1024),
        decay_cache,
    )


def shards(
    tokens, mix_gain, w_query, w_key, w_value, w_forget, query_gain,
    key_cache, value_cache, decay_cache, w_out, mlp_gain, w_up, w_down,
):
    shape = jax.ShapeDtypeStruct
    head = call(head_kernel, shape((8, 128), F32), "head", cost=3 * 10**9)()
    operands = (tokens, mix_gain.reshape(1, -1), w_query, w_key.T, w_value.T, w_forget.T)
    query, extra = call(project_kernel, (shape((64, 256), BF), shape((64, 256), BF)), "project")(head, *operands)
    message = call(spread_kernel, shape((16, 72, 256), BF), "spread", cost=10**10)(query, extra)
    message = exchange(message, "kv")
    part = attend(message, query_gain, key_cache, value_cache, decay_cache)
    partial = call(merge_kernel, shape((64, 256), BF), "merge")(sent(part, "kv"), w_out)
    residual, message = call(up_kernel, (shape((64, 256), BF), shape((16, 72, 128), BF)), "up")(
        pair_sum(partial), tokens, mlp_gain.reshape(1, -1), w_up
    )
    message = call(hidden_kernel, shape((16, 64, 128), BF), "hidden")(exchange(message, "kv"))
    partial = call(down_kernel, shape((64, 256), BF), "down")(exchange(message, "kv"), w_down)
    return call(finish_kernel, shape((64, 256), BF), "finish")(pair_sum(partial), residual)


def solution(mesh):
    split = Mesh(mesh.devices.reshape(mesh.shape["kv"], -1, 2), ("kv", "x", "core"))
    return jax.shard_map(
        shards,
        mesh=split,
        in_specs=(
            P(None, "kv"),
            P("kv"),
            P("kv", TP),
            P("kv", TP),
            P("kv", TP),
            P("kv", TP),
            P(),
            P(None, TP, None, "kv"),
            P(None, TP, None, "kv"),
            P(None, TP, "kv"),
            P(TP, "kv"),
            P("kv"),
            P("kv", TP),
            P(TP, "kv"),
        ),
        out_specs=P(None, "kv"),
        check_vma=False,
    )
```

```python
import jax
import jax.numpy as jnp
from jax import lax
from jax.experimental import pallas as pl
from jax.experimental.pallas import tpu as pltpu
from jax.sharding import Mesh
from jax.sharding import PartitionSpec as P

D = 4096
HEAD_DIM = 64
EPS = 1e-06
TP = ("x", "core")
BF = jnp.bfloat16
F32 = jnp.float32

VM = pl.BlockSpec(memory_space=pltpu.VMEM)


def iota(shape, dim):
    return lax.broadcasted_iota(jnp.int32, shape, dim)


def dot(a, b):
    return jnp.dot(a, b, preferred_element_type=F32)


def dot_t(a, b):
    return lax.dot_general(a, b, (((1,), (1,)), ((), ())), preferred_element_type=F32)


def high(a):
    return a.astype(BF).astype(F32)


def column_to_row(column, width, at):
    n = column.shape[0]
    place = iota((n, width), 1) == iota((n, width), 0) + at
    return jnp.sum(jnp.where(place, column, 0.0), axis=0, keepdims=True)


def row_to_column(row, n, at):
    width = row.shape[1]
    place = iota((n, width), 1) == iota((n, width), 0) + at
    return jnp.sum(jnp.where(place, row, 0.0), axis=1, keepdims=True)


def call(kernel, outs, name, scratch=(), in_specs=None, limit=16 << 20, cost=None):
    def run(*args):
        return pl.pallas_call(
            kernel,
            out_shape=outs,
            in_specs=in_specs or [VM] * len(args),
            out_specs=jax.tree.map(lambda _: VM, outs),
            scratch_shapes=list(scratch),
            compiler_params=pltpu.CompilerParams(vmem_limit_bytes=limit),
            name=name,
            cost_estimate=cost and pl.CostEstimate(flops=cost, bytes_accessed=cost // 100, transcendentals=0),
        )(*args)

    return run


def project_kernel(head, tokens, gain, w_query, w_key, w_value, w_forget, query_out, extra_out):
    stream = tokens[...].astype(F32)
    squares = jnp.sum(stream * stream, axis=1, keepdims=True)
    normed = (stream * gain[...]).astype(BF)
    query_out[...] = dot(normed, w_query[...]).astype(BF)
    key_value = dot_t(normed, jnp.concatenate([w_key[...], w_value[...]], axis=0))
    forget_w = w_forget[...].astype(F32)
    forget_w = jnp.concatenate([forget_w, forget_w, jnp.zeros((120, 256), F32)], axis=0)
    forget = dot_t(normed, forget_w.astype(BF))
    forget = jnp.where(iota(forget.shape, 1) < 4, high(forget), forget - high(forget))
    squares_high = high(squares)
    row_high = column_to_row(squares_high, 128, 64)
    row_low = column_to_row(squares - squares_high, 128, 64)
    line = iota((64, 128), 0) % 4
    forget = forget + jnp.where(line == 0, row_high, jnp.where(line == 1, row_low, 0.0))
    upper = iota((8, 128), 0) < 4
    for p in range(16):
        rows = slice(8 * (p // 2), 8 * (p // 2) + 8)
        first, second = key_value[rows], forget[rows]
        if p % 2 == 0:
            second = pltpu.roll(second, 4, 0)
        else:
            first = pltpu.roll(first, 4, 0)
        extra_out[8 * p : 8 * p + 8, :] = jnp.where(upper, first, second).astype(BF)


def head_kernel(out):
    out[...] = jnp.zeros_like(out)


def spread_kernel(query, extra, out):
    for p in range(16):
        out[p, 0:64, :] = query[:, 0:128]
        out[p, 64:128, :] = query[:, 128:256]
        out[p, 128:136, :] = extra[8 * p : 8 * p + 8, :]


def attend_kernel(
    parts, query_gain, keys, values, decay, out,
    scales, query_rows, left, peaks, masses,
):
    total = [parts[i].astype(F32) for i in range(16)]
    while len(total) > 1:
        total = [a + b for a, b in zip(total[::2], total[1::2])]
    raw = jnp.concatenate([total[0][0:64], total[0][64:128]], axis=1)
    extra = total[0][128:136]
    squares = row_to_column(extra[4:5] + extra[5:6], 64, 64)
    scale = lax.rsqrt(squares / D + EPS)
    scales[...] = jnp.broadcast_to(scale, (64, 128))
    head_of = iota((64, 256), 1) // HEAD_DIM
    power = raw * raw
    inverse = jnp.zeros((64, 256), F32)
    for h in range(4):
        mean = jnp.sum(jnp.where(head_of == h, power, 0.0), axis=1, keepdims=True) / HEAD_DIM
        inverse = jnp.where(head_of == h, scale * lax.rsqrt(scale * scale * mean + EPS), inverse)
    gain = query_gain[...]
    gain = jnp.concatenate([gain, gain, gain, gain], axis=1)
    query = (raw * inverse * gain).astype(BF)

    repeat = (iota((256, 64), 0) // 4 == iota((256, 64), 1)).astype(BF)
    spread = dot(repeat, query)
    own_lanes = iota((256, 256), 1) // HEAD_DIM == iota((256, 256), 0) % 4
    spread = jnp.where(own_lanes, spread, 0.0)
    folded = spread[:, 0:128] + spread[:, 128:256]
    folded = folded + pltpu.roll(folded, 64, 1)
    query_rows[...] = folded
    wide = jnp.concatenate([folded] * 2, axis=1)
    block = iota((256, 256), 1) // HEAD_DIM == (iota((256, 256), 0) // 4) % 4
    left[...] = jnp.where(block, wide * (HEAD_DIM ** (-0.5)), 0.0).astype(BF)

    me = lax.axis_index("kv")
    own_scale = scales[pl.ds(pl.multiple_of(8 * (me // 2), 8), 8), :]
    own_scale = jnp.where(me % 2 == 0, own_scale, pltpu.roll(own_scale, 4, 0))
    key_value = (own_scale * extra).astype(BF)
    forget = pltpu.roll(extra, 4, 0)
    forget = own_scale * (forget + pltpu.roll(forget, 124, 1))
    log_forget = -(jnp.maximum(-forget, 0.0) + jnp.log1p(jnp.exp(-jnp.abs(forget))))
    log_forget = jnp.where((iota((8, 128), 1) < 4) & (iota((8, 128), 0) < 4), log_forget, 0.0)
    repeat4 = iota((128, 8), 0) // 4 % 4 == iota((128, 8), 1)
    key_value = dot(repeat4.astype(BF), key_value)
    log_forget = jnp.dot(
        repeat4[0:16].astype(F32), log_forget, preferred_element_type=F32, precision=lax.Precision.HIGHEST
    )
    mine = iota((16, 128), 1) == iota((16, 128), 0) % 4
    log_forget = jnp.sum(jnp.where(mine, log_forget, 0.0), axis=1, keepdims=True)
    at = pl.ds(pl.multiple_of(16 * me, 16), 16)
    lower = iota((16, 128), 1) < 64
    own = jnp.sum(jnp.where(lower, query_rows[at, :] * key_value[0:16], 0.0), axis=1, keepdims=True)
    own = own * (HEAD_DIM ** (-0.5)) - log_forget
    own = jnp.concatenate([own] * 8, axis=0)
    place = iota((128, 128), 0) == iota((128, 128), 1)
    own = jnp.sum(jnp.where(place, own, 0.0), axis=0, keepdims=True)
    pick = (iota((64, 128), 1) == iota((64, 128), 0) + 64).astype(BF)
    value = dot_t(pick, key_value.astype(BF))

    lane = iota((64, 16), 1)
    folds = []
    def score(g):
        scores = dot(left[16 * g : 16 * g + 16, :], keys[256 * g : 256 * g + 256, :])
        return scores + decay[4 * g : 4 * g + 4].reshape(16, 1024)

    ahead = [score(g) for g in range(8)]
    for g in range(16):
        rows = slice(16 * g, 16 * g + 16)
        scores = ahead.pop(0)
        peak = jnp.max(scores, axis=1, keepdims=True)
        weights = jnp.exp(scores - peak)
        mass = jnp.sum(weights, axis=1, keepdims=True)
        peaks[rows, :] = jnp.broadcast_to(peak, (16, 128))
        masses[rows, :] = jnp.broadcast_to(mass, (16, 128))
        weights = weights.astype(BF)
        if g + 8 < 16:
            ahead.append(score(g + 8))
        summed = dot_t(values[256 * g : 256 * g + 256, :], weights)
        total = summed[0:64]
        for k in range(1, 4):
            total = jnp.where(lane // 4 == k, summed[64 * k : 64 * k + 64], total)
        folds.append(total)
    sums = [jnp.concatenate(folds[8 * j : 8 * j + 8], axis=1) for j in range(2)]

    line = iota((8, 128), 0)
    slot = iota((1, 128), 1) // 16
    packed = jnp.zeros((8, 128), F32)
    for j in range(2):
        rows = slice(128 * j, 128 * j + 128)
        peak = jnp.sum(jnp.where(place, peaks[rows, :], 0.0), axis=0, keepdims=True)
        mass = jnp.sum(jnp.where(place, masses[rows, :], 0.0), axis=0, keepdims=True)
        joined = jnp.where(slot + 8 * j == me, own, peak - 1e30)
        top = jnp.maximum(peak, joined)
        keep = jnp.exp(peak - top)
        weight = jnp.exp(joined - top)
        mass = mass * keep + weight
        out[64 * j : 64 * j + 64, :] = ((sums[j] * keep + high(weight) * value) / mass).astype(BF)
        level = top + jnp.log(mass)
        for k in range(3):
            piece = high(level)
            packed = jnp.where(line == 3 * j + k, piece, packed)
            level = level - piece
    out[128:136, :] = packed.astype(BF)


def merge_kernel(parts, w_out, out):
    extra = parts[:, 128:136, :].astype(F32)
    row, column = iota((128, 128), 0), iota((128, 128), 1)
    order = ((row % 32 == column // 4) & (row // 32 == column % 4)).astype(BF)
    heads = []
    for j in range(2):
        level = extra[:, 3 * j, :] + extra[:, 3 * j + 1, :] + extra[:, 3 * j + 2, :]
        factor = jnp.exp(level - jnp.max(level, axis=0, keepdims=True))
        factor = factor / jnp.sum(factor, axis=0, keepdims=True)
        total = jnp.zeros((64, 128), F32)
        for i in range(16):
            total = total + parts[i, 64 * j : 64 * j + 64, :].astype(F32) * factor[i : i + 1, :]
        heads.append(dot_t(order, total.astype(BF)).astype(BF))
    partial = jnp.zeros((64, 256), F32)
    for h in range(4):
        attended = jnp.concatenate([heads[0][32 * h : 32 * h + 32], heads[1][32 * h : 32 * h + 32]], axis=0)
        partial = partial + dot(attended, w_out[64 * h : 64 * h + 64, :])
    out[...] = partial.astype(BF)


def pair_kernel(mine, partner, out):
    total = (mine[...].astype(F32) + partner[...].astype(F32)).astype(BF)
    for i in range(4):
        out[i] = total


def up_kernel(parts, tokens, gain, w_up, residual_out, out):
    attn = parts[0].astype(F32)
    for i in range(1, 4):
        attn = attn + parts[i].astype(F32)
    residual = (tokens[...].astype(F32) + high(attn)).astype(BF)
    residual_out[...] = residual
    wide = residual.astype(F32)
    squares = jnp.sum(wide * wide, axis=1, keepdims=True)
    squares_high = high(squares)
    row_high = column_to_row(squares_high, 128, 0)
    row_low = column_to_row(squares - squares_high, 128, 0)
    line = iota((8, 128), 0)
    tile = jnp.where(line == 0, row_high, jnp.where(line == 1, row_low, 0.0)).astype(BF)
    normed = (wide * gain[...]).astype(BF)
    for p in range(0, 16, 2):
        up = dot(normed, w_up[:, 128 * p : 128 * p + 256]).astype(BF)
        for k in range(2):
            out[p + k, 0:64, :] = up[:, 128 * k : 128 * k + 128]
            out[p + k, 64:72, :] = tile


def hidden_kernel(parts, out):
    up = parts[0, 0:64, :].astype(F32)
    extra = parts[0, 64:72, :].astype(F32)
    for i in range(1, 16):
        up = up + parts[i, 0:64, :].astype(F32)
        extra = extra + parts[i, 64:72, :].astype(F32)
    squares = row_to_column(extra[0:1] + extra[1:2], 64, 0)
    up = lax.rsqrt(squares / D + EPS) * up
    up = jnp.maximum(up, 0.0)
    hidden = (up * up).astype(BF)
    for i in range(16):
        out[i] = hidden


def down_kernel(parts, w_down, out):
    down = jnp.zeros((64, 256), F32)
    for i in range(0, 16, 2):
        pair = jnp.concatenate([parts[i], parts[i + 1]], axis=1)
        down = down + dot(pair, w_down[128 * i : 128 * i + 256, :])
    out[...] = down.astype(BF)


def finish_kernel(parts, residual, out):
    down = parts[0].astype(F32)
    for i in range(1, 4):
        down = down + parts[i].astype(F32)
    out[...] = (residual[...].astype(F32) + high(down)).astype(BF)


def exchange(array, axis):
    return lax.all_to_all(array, axis, split_axis=0, concat_axis=0, tiled=True)


def pair_sum(partial):
    partner = lax.ppermute(partial, "core", [(0, 1), (1, 0)])
    message = call(pair_kernel, jax.ShapeDtypeStruct((4, 64, 256), BF), "pair")(partial, partner)
    return exchange(message, "x")


def sent(array, axis):
    return exchange(jnp.broadcast_to(array, (lax.axis_size(axis), *array.shape)), axis)


def attend(message, query_gain, key_cache, value_cache, decay_cache):
    return call(
        attend_kernel,
        jax.ShapeDtypeStruct((136, 128), BF),
        "attend",
        scratch=[
            pltpu.VMEM((64, 128), F32),
            pltpu.VMEM((256, 128), F32),
            pltpu.VMEM((256, 256), BF),
            pltpu.VMEM((256, 128), F32),
            pltpu.VMEM((256, 128), F32),
        ],
        limit=8 << 20,
    )(
        message,
        query_gain.reshape(1, -1),
        key_cache.reshape(4096, 1024),
        value_cache.reshape(4096, 1024),
        decay_cache,
    )


def shards(
    tokens, mix_gain, w_query, w_key, w_value, w_forget, query_gain,
    key_cache, value_cache, decay_cache, w_out, mlp_gain, w_up, w_down,
):
    shape = jax.ShapeDtypeStruct
    head = call(head_kernel, shape((8, 128), F32), "head", cost=3 * 10**9)()
    operands = (tokens, mix_gain.reshape(1, -1), w_query, w_key.T, w_value.T, w_forget.T)
    query, extra = call(project_kernel, (shape((64, 256), BF), shape((128, 128), BF)), "project")(head, *operands)
    message = call(spread_kernel, shape((16, 136, 128), BF), "spread", cost=10**10)(query, extra)
    message = exchange(message, "kv")
    part = attend(message, query_gain, key_cache, value_cache, decay_cache)
    partial = call(merge_kernel, shape((64, 256), BF), "merge")(sent(part, "kv"), w_out)
    residual, message = call(up_kernel, (shape((64, 256), BF), shape((16, 72, 128), BF)), "up")(
        pair_sum(partial), tokens, mlp_gain.reshape(1, -1), w_up
    )
    message = call(hidden_kernel, shape((16, 64, 128), BF), "hidden")(exchange(message, "kv"))
    partial = call(down_kernel, shape((64, 256), BF), "down")(exchange(message, "kv"), w_down)
    return call(finish_kernel, shape((64, 256), BF), "finish")(pair_sum(partial), residual)


def solution(mesh):
    split = Mesh(mesh.devices.reshape(mesh.shape["kv"], -1, 2), ("kv", "x", "core"))
    return jax.shard_map(
        shards,
        mesh=split,
        in_specs=(
            P(None, "kv"),
            P("kv"),
            P("kv", TP),
            P("kv", TP),
            P("kv", TP),
            P("kv", TP),
            P(),
            P(None, TP, None, "kv"),
            P(None, TP, None, "kv"),
            P(None, TP, "kv"),
            P(TP, "kv"),
            P("kv"),
            P("kv", TP),
            P(TP, "kv"),
        ),
        out_specs=P(None, "kv"),
        check_vma=False,
    )
```

```python
import jax
import jax.numpy as jnp
from jax import lax
from jax.experimental import pallas as pl
from jax.experimental.pallas import tpu as pltpu
from jax.sharding import Mesh
from jax.sharding import PartitionSpec as P

D = 4096
HEAD_DIM = 64
EPS = 1e-06
TP = ("x", "core")
BF = jnp.bfloat16
F32 = jnp.float32

VM = pl.BlockSpec(memory_space=pltpu.VMEM)


def iota(shape, dim):
    return lax.broadcasted_iota(jnp.int32, shape, dim)


def dot(a, b):
    return jnp.dot(a, b, preferred_element_type=F32)


def dot_t(a, b):
    return lax.dot_general(a, b, (((1,), (1,)), ((), ())), preferred_element_type=F32)


def high(a):
    return a.astype(BF).astype(F32)


def column_to_row(column, width, at):
    n = column.shape[0]
    place = iota((n, width), 1) == iota((n, width), 0) + at
    return jnp.sum(jnp.where(place, column, 0.0), axis=0, keepdims=True)


def row_to_column(row, n, at):
    width = row.shape[1]
    place = iota((n, width), 1) == iota((n, width), 0) + at
    return jnp.sum(jnp.where(place, row, 0.0), axis=1, keepdims=True)


def call(kernel, outs, name, scratch=(), in_specs=None, limit=16 << 20, cost=None):
    def run(*args):
        return pl.pallas_call(
            kernel,
            out_shape=outs,
            in_specs=in_specs or [VM] * len(args),
            out_specs=jax.tree.map(lambda _: VM, outs),
            scratch_shapes=list(scratch),
            compiler_params=pltpu.CompilerParams(vmem_limit_bytes=limit),
            name=name,
            cost_estimate=cost and pl.CostEstimate(flops=cost, bytes_accessed=cost // 100, transcendentals=0),
        )(*args)

    return run


def project_kernel(head, tokens, gain, w_query, w_key, w_value, w_forget, query_out, extra_out):
    stream = tokens[...].astype(F32)
    squares = jnp.sum(stream * stream, axis=1, keepdims=True)
    normed = (stream * gain[...]).astype(BF)
    query_out[...] = dot(normed, w_query[...]).astype(BF)
    key_value = dot_t(normed, jnp.concatenate([w_key[...], w_value[...]], axis=0))
    forget_w = w_forget[...].astype(F32)
    forget_w = jnp.concatenate([forget_w, forget_w, jnp.zeros((120, 256), F32)], axis=0)
    forget = dot_t(normed, forget_w.astype(BF))
    forget = jnp.where(iota(forget.shape, 1) < 4, high(forget), forget - high(forget))
    squares_high = high(squares)
    row_high = column_to_row(squares_high, 128, 64)
    row_low = column_to_row(squares - squares_high, 128, 64)
    line = iota((64, 128), 0) % 4
    forget = forget + jnp.where(line == 0, row_high, jnp.where(line == 1, row_low, 0.0))
    upper = iota((8, 128), 0) < 4
    for p in range(16):
        rows = slice(8 * (p // 2), 8 * (p // 2) + 8)
        first, second = key_value[rows], forget[rows]
        if p % 2 == 0:
            second = pltpu.roll(second, 4, 0)
        else:
            first = pltpu.roll(first, 4, 0)
        extra_out[8 * p : 8 * p + 8, :] = jnp.where(upper, first, second).astype(BF)


def head_kernel(out):
    out[...] = jnp.zeros_like(out)


def spread_kernel(query, extra, out):
    for p in range(16):
        out[p, 0:64, :] = query[:, 0:128]
        out[p, 64:128, :] = query[:, 128:256]
        out[p, 128:136, :] = extra[8 * p : 8 * p + 8, :]


def attend_kernel(
    parts, query_gain, keys, values, decay, out,
    scales, query_rows, peaks, masses,
):
    total = [parts[i].astype(F32) for i in range(16)]
    while len(total) > 1:
        total = [a + b for a, b in zip(total[::2], total[1::2])]
    raw = jnp.concatenate([total[0][0:64], total[0][64:128]], axis=1)
    extra = total[0][128:136]
    squares = row_to_column(extra[4:5] + extra[5:6], 64, 64)
    scale = lax.rsqrt(squares / D + EPS)
    scales[...] = jnp.broadcast_to(scale, (64, 128))
    head_of = iota((64, 256), 1) // HEAD_DIM
    power = raw * raw
    inverse = jnp.zeros((64, 256), F32)
    for h in range(4):
        half = power[:, 128 * (h // 2) : 128 * (h // 2) + 128]
        half = jnp.where(iota((64, 128), 1) // HEAD_DIM == h % 2, half, 0.0)
        mean = jnp.sum(half, axis=1, keepdims=True) / HEAD_DIM
        inverse = jnp.where(head_of == h, scale * lax.rsqrt(scale * scale * mean + EPS), inverse)
    gain = query_gain[...]
    gain = jnp.concatenate([gain, gain, gain, gain], axis=1)
    query = (raw * inverse * gain).astype(BF)

    repeat = (iota((256, 64), 0) // 4 == iota((256, 64), 1)).astype(BF)
    spread = dot(repeat, query)
    own_lanes = iota((256, 256), 1) // HEAD_DIM == iota((256, 256), 0) % 4
    spread = jnp.where(own_lanes, spread, 0.0)
    folded = spread[:, 0:128] + spread[:, 128:256]
    folded = folded + pltpu.roll(folded, 64, 1)
    query_rows[...] = folded
    wide = jnp.concatenate([folded] * 2, axis=1)
    block = iota((256, 256), 1) // HEAD_DIM == (iota((256, 256), 0) // 4) % 4
    left = jnp.where(block, wide * (HEAD_DIM ** (-0.5)), 0.0).astype(BF)

    me = lax.axis_index("kv")
    own_scale = scales[pl.ds(pl.multiple_of(8 * (me // 2), 8), 8), :]
    own_scale = jnp.where(me % 2 == 0, own_scale, pltpu.roll(own_scale, 4, 0))
    key_value = (own_scale * extra).astype(BF)
    forget = pltpu.roll(extra, 4, 0)
    forget = own_scale * (forget + pltpu.roll(forget, 124, 1))
    log_forget = -(jnp.maximum(-forget, 0.0) + jnp.log1p(jnp.exp(-jnp.abs(forget))))
    log_forget = jnp.where((iota((8, 128), 1) < 4) & (iota((8, 128), 0) < 4), log_forget, 0.0)
    repeat4 = iota((128, 8), 0) // 4 % 4 == iota((128, 8), 1)
    key_value = dot(repeat4.astype(BF), key_value)
    log_forget = jnp.dot(
        repeat4[0:16].astype(F32), log_forget, preferred_element_type=F32, precision=lax.Precision.HIGHEST
    )
    mine = iota((16, 128), 1) == iota((16, 128), 0) % 4
    log_forget = jnp.sum(jnp.where(mine, log_forget, 0.0), axis=1, keepdims=True)
    at = pl.ds(pl.multiple_of(16 * me, 16), 16)
    lower = iota((16, 128), 1) < 64
    own = jnp.sum(jnp.where(lower, query_rows[at, :] * key_value[0:16], 0.0), axis=1, keepdims=True)
    own = own * (HEAD_DIM ** (-0.5)) - log_forget
    own = jnp.concatenate([own] * 8, axis=0)
    place = iota((128, 128), 0) == iota((128, 128), 1)
    own = jnp.sum(jnp.where(place, own, 0.0), axis=0, keepdims=True)
    pick = (iota((64, 128), 1) == iota((64, 128), 0) + 64).astype(BF)
    value = dot_t(pick, key_value.astype(BF))

    lane = iota((64, 16), 1)
    folds = []
    def score(g):
        scores = dot(left[16 * g : 16 * g + 16], keys[256 * g : 256 * g + 256, :])
        return scores + decay[4 * g : 4 * g + 4].reshape(16, 1024)

    ahead = [score(g) for g in range(8)]
    for g in range(16):
        rows = slice(16 * g, 16 * g + 16)
        scores = ahead.pop(0)
        peak = jnp.max(scores, axis=1, keepdims=True)
        weights = jnp.exp(scores - peak)
        mass = jnp.sum(weights, axis=1, keepdims=True)
        peaks[rows, :] = jnp.broadcast_to(peak, (16, 128))
        masses[rows, :] = jnp.broadcast_to(mass, (16, 128))
        weights = weights.astype(BF)
        if g + 8 < 16:
            ahead.append(score(g + 8))
        summed = dot_t(values[256 * g : 256 * g + 256, :], weights)
        total = summed[0:64]
        for k in range(1, 4):
            total = jnp.where(lane // 4 == k, summed[64 * k : 64 * k + 64], total)
        folds.append(total)
    sums = [jnp.concatenate(folds[8 * j : 8 * j + 8], axis=1) for j in range(2)]

    line = iota((8, 128), 0)
    slot = iota((1, 128), 1) // 16
    packed = jnp.zeros((8, 128), F32)
    for j in range(2):
        rows = slice(128 * j, 128 * j + 128)
        peak = jnp.sum(jnp.where(place, peaks[rows, :], 0.0), axis=0, keepdims=True)
        mass = jnp.sum(jnp.where(place, masses[rows, :], 0.0), axis=0, keepdims=True)
        joined = jnp.where(slot + 8 * j == me, own, peak - 1e30)
        top = jnp.maximum(peak, joined)
        keep = jnp.exp(peak - top)
        weight = jnp.exp(joined - top)
        mass = mass * keep + weight
        result = ((sums[j] * keep + high(weight) * value) / mass).astype(BF)
        for i in range(16):
            out[i, 64 * j : 64 * j + 64, :] = result
        level = top + jnp.log(mass)
        for k in range(3):
            piece = high(level)
            packed = jnp.where(line == 3 * j + k, piece, packed)
            level = level - piece
    packed = packed.astype(BF)
    for i in range(16):
        out[i, 128:136, :] = packed


def merge_kernel(parts, w_out, out):
    extra = parts[:, 128:136, :].astype(F32)
    row, column = iota((128, 128), 0), iota((128, 128), 1)
    order = ((row % 32 == column // 4) & (row // 32 == column % 4)).astype(BF)
    heads = []
    for j in range(2):
        level = extra[:, 3 * j, :] + extra[:, 3 * j + 1, :] + extra[:, 3 * j + 2, :]
        factor = jnp.exp(level - jnp.max(level, axis=0, keepdims=True))
        factor = factor / jnp.sum(factor, axis=0, keepdims=True)
        total = jnp.zeros((64, 128), F32)
        for i in range(16):
            total = total + parts[i, 64 * j : 64 * j + 64, :].astype(F32) * factor[i : i + 1, :]
        heads.append(dot_t(order, total.astype(BF)).astype(BF))
    partial = jnp.zeros((64, 256), F32)
    for h in range(4):
        attended = jnp.concatenate([heads[0][32 * h : 32 * h + 32], heads[1][32 * h : 32 * h + 32]], axis=0)
        partial = partial + dot(attended, w_out[64 * h : 64 * h + 64, :])
    out[...] = partial.astype(BF)


def pair_kernel(mine, partner, out):
    total = (mine[...].astype(F32) + partner[...].astype(F32)).astype(BF)
    for i in range(4):
        out[i] = total


def up_kernel(parts, tokens, gain, w_up, residual_out, out):
    attn = parts[0].astype(F32)
    for i in range(1, 4):
        attn = attn + parts[i].astype(F32)
    residual = (tokens[...].astype(F32) + high(attn)).astype(BF)
    residual_out[...] = residual
    wide = residual.astype(F32)
    squares = jnp.sum(wide * wide, axis=1, keepdims=True)
    squares_high = high(squares)
    row_high = column_to_row(squares_high, 128, 0)
    row_low = column_to_row(squares - squares_high, 128, 0)
    line = iota((8, 128), 0)
    tile = jnp.where(line == 0, row_high, jnp.where(line == 1, row_low, 0.0)).astype(BF)
    normed = (wide * gain[...]).astype(BF)
    for p in range(0, 16, 2):
        up = dot(normed, w_up[:, 128 * p : 128 * p + 256]).astype(BF)
        for k in range(2):
            out[p + k, 0:64, :] = up[:, 128 * k : 128 * k + 128]
            out[p + k, 64:72, :] = tile


def hidden_kernel(parts, out):
    up = parts[0, 0:64, :].astype(F32)
    extra = parts[0, 64:72, :].astype(F32)
    for i in range(1, 16):
        up = up + parts[i, 0:64, :].astype(F32)
        extra = extra + parts[i, 64:72, :].astype(F32)
    squares = row_to_column(extra[0:1] + extra[1:2], 64, 0)
    up = lax.rsqrt(squares / D + EPS) * up
    up = jnp.maximum(up, 0.0)
    hidden = (up * up).astype(BF)
    for i in range(16):
        out[i] = hidden


def down_kernel(parts, w_down, out):
    down = jnp.zeros((64, 256), F32)
    for i in range(0, 16, 2):
        pair = jnp.concatenate([parts[i], parts[i + 1]], axis=1)
        down = down + dot(pair, w_down[128 * i : 128 * i + 256, :])
    out[...] = down.astype(BF)


def finish_kernel(parts, residual, out):
    down = parts[0].astype(F32)
    for i in range(1, 4):
        down = down + parts[i].astype(F32)
    out[...] = (residual[...].astype(F32) + high(down)).astype(BF)


def exchange(array, axis):
    return lax.all_to_all(array, axis, split_axis=0, concat_axis=0, tiled=True)


def pair_sum(partial):
    partner = lax.ppermute(partial, "core", [(0, 1), (1, 0)])
    message = call(pair_kernel, jax.ShapeDtypeStruct((4, 64, 256), BF), "pair")(partial, partner)
    return exchange(message, "x")


def attend(message, query_gain, key_cache, value_cache, decay_cache):
    return call(
        attend_kernel,
        jax.ShapeDtypeStruct((16, 136, 128), BF),
        "attend",
        scratch=[
            pltpu.VMEM((64, 128), F32),
            pltpu.VMEM((256, 128), F32),
            pltpu.VMEM((256, 128), F32),
            pltpu.VMEM((256, 128), F32),
        ],
        limit=8 << 20,
    )(
        message,
        query_gain.reshape(1, -1),
        key_cache.reshape(4096, 1024),
        value_cache.reshape(4096, 1024),
        decay_cache,
    )


def shards(
    tokens, mix_gain, w_query, w_key, w_value, w_forget, query_gain,
    key_cache, value_cache, decay_cache, w_out, mlp_gain, w_up, w_down,
):
    shape = jax.ShapeDtypeStruct
    head = call(head_kernel, shape((8, 128), F32), "head", cost=3 * 10**9)()
    operands = (tokens, mix_gain.reshape(1, -1), w_query, w_key.T, w_value.T, w_forget.T)
    query, extra = call(project_kernel, (shape((64, 256), BF), shape((128, 128), BF)), "project")(head, *operands)
    message = call(spread_kernel, shape((16, 136, 128), BF), "spread", cost=10**10)(query, extra)
    message = exchange(message, "kv")
    part = attend(message, query_gain, key_cache, value_cache, decay_cache)
    partial = call(merge_kernel, shape((64, 256), BF), "merge")(exchange(part, "kv"), w_out)
    residual, message = call(up_kernel, (shape((64, 256), BF), shape((16, 72, 128), BF)), "up")(
        pair_sum(partial), tokens, mlp_gain.reshape(1, -1), w_up
    )
    message = call(hidden_kernel, shape((16, 64, 128), BF), "hidden")(exchange(message, "kv"))
    partial = call(down_kernel, shape((64, 256), BF), "down")(exchange(message, "kv"), w_down)
    return call(finish_kernel, shape((64, 256), BF), "finish")(pair_sum(partial), residual)


def solution(mesh):
    split = Mesh(mesh.devices.reshape(mesh.shape["kv"], -1, 2), ("kv", "x", "core"))
    return jax.shard_map(
        shards,
        mesh=split,
        in_specs=(
            P(None, "kv"),
            P("kv"),
            P("kv", TP),
            P("kv", TP),
            P("kv", TP),
            P("kv", TP),
            P(),
            P(None, TP, None, "kv"),
            P(None, TP, None, "kv"),
            P(None, TP, "kv"),
            P(TP, "kv"),
            P("kv"),
            P("kv", TP),
            P(TP, "kv"),
        ),
        out_specs=P(None, "kv"),
        check_vma=False,
    )
```

```python
import jax
import jax.numpy as jnp
from jax import lax
from jax.experimental import pallas as pl
from jax.experimental.pallas import tpu as pltpu
from jax.sharding import Mesh
from jax.sharding import PartitionSpec as P

D = 4096
HEAD_DIM = 64
EPS = 1e-06
TP = ("x", "core")
BF = jnp.bfloat16
F32 = jnp.float32

VM = pl.BlockSpec(memory_space=pltpu.VMEM)


def iota(shape, dim):
    return lax.broadcasted_iota(jnp.int32, shape, dim)


def dot(a, b):
    return jnp.dot(a, b, preferred_element_type=F32)


def dot_t(a, b):
    return lax.dot_general(a, b, (((1,), (1,)), ((), ())), preferred_element_type=F32)


def high(a):
    return a.astype(BF).astype(F32)


def column_to_row(column, width, at):
    n = column.shape[0]
    place = iota((n, width), 1) == iota((n, width), 0) + at
    return jnp.sum(jnp.where(place, column, 0.0), axis=0, keepdims=True)


def row_to_column(row, n, at):
    width = row.shape[1]
    place = iota((n, width), 1) == iota((n, width), 0) + at
    return jnp.sum(jnp.where(place, row, 0.0), axis=1, keepdims=True)


def call(kernel, outs, name, scratch=(), in_specs=None, limit=16 << 20, cost=None):
    def run(*args):
        return pl.pallas_call(
            kernel,
            out_shape=outs,
            in_specs=in_specs or [VM] * len(args),
            out_specs=jax.tree.map(lambda _: VM, outs),
            scratch_shapes=list(scratch),
            compiler_params=pltpu.CompilerParams(vmem_limit_bytes=limit),
            name=name,
            cost_estimate=cost and pl.CostEstimate(flops=cost, bytes_accessed=cost // 100, transcendentals=0),
        )(*args)

    return run


def project_kernel(head, tokens, gain, w_query, w_key, w_value, w_forget, query_out, extra_out):
    stream = tokens[...].astype(F32)
    squares = jnp.sum(stream * stream, axis=1, keepdims=True)
    normed = (stream * gain[...]).astype(BF)
    query_out[...] = dot(normed, w_query[...]).astype(BF)
    key_value = dot_t(normed, jnp.concatenate([w_key[...], w_value[...]], axis=0))
    forget_w = w_forget[...].astype(F32)
    forget_w = jnp.concatenate([forget_w, forget_w, jnp.zeros((120, 256), F32)], axis=0)
    forget = dot_t(normed, forget_w.astype(BF))
    forget = jnp.where(iota(forget.shape, 1) < 4, high(forget), forget - high(forget))
    squares_high = high(squares)
    row_high = column_to_row(squares_high, 128, 64)
    row_low = column_to_row(squares - squares_high, 128, 64)
    line = iota((64, 128), 0) % 4
    forget = forget + jnp.where(line == 0, row_high, jnp.where(line == 1, row_low, 0.0))
    upper = iota((8, 128), 0) < 4
    for p in range(16):
        rows = slice(8 * (p // 2), 8 * (p // 2) + 8)
        first, second = key_value[rows], forget[rows]
        if p % 2 == 0:
            second = pltpu.roll(second, 4, 0)
        else:
            first = pltpu.roll(first, 4, 0)
        extra_out[8 * p : 8 * p + 8, :] = jnp.where(upper, first, second).astype(BF)


def head_kernel(out):
    out[...] = jnp.zeros_like(out)


def spread_kernel(query, extra, out):
    for p in range(16):
        out[p, 0:64, :] = query[:, 0:128]
        out[p, 64:128, :] = query[:, 128:256]
        out[p, 128:136, :] = extra[8 * p : 8 * p + 8, :]


def attend_kernel(
    parts, query_gain, keys, values, decay, out,
    scales, query_rows, peaks, masses,
):
    total = [parts[i].astype(F32) for i in range(16)]
    while len(total) > 1:
        total = [a + b for a, b in zip(total[::2], total[1::2])]
    raw = jnp.concatenate([total[0][0:64], total[0][64:128]], axis=1)
    extra = total[0][128:136]
    squares = row_to_column(extra[4:5] + extra[5:6], 64, 64)
    scale = lax.rsqrt(squares / D + EPS)
    scales[...] = jnp.broadcast_to(scale, (64, 128))
    head_of = iota((64, 256), 1) // HEAD_DIM
    power = raw * raw
    inverse = jnp.zeros((64, 256), F32)
    for h in range(4):
        half = power[:, 128 * (h // 2) : 128 * (h // 2) + 128]
        half = jnp.where(iota((64, 128), 1) // HEAD_DIM == h % 2, half, 0.0)
        mean = jnp.sum(half, axis=1, keepdims=True) / HEAD_DIM
        inverse = jnp.where(head_of == h, scale * lax.rsqrt(scale * scale * mean + EPS), inverse)
    gain = query_gain[...]
    gain = jnp.concatenate([gain, gain, gain, gain], axis=1)
    query = (raw * inverse * gain).astype(BF)

    repeat = (iota((256, 64), 0) // 4 == iota((256, 64), 1)).astype(BF)
    spread = dot(repeat, query)
    own_lanes = iota((256, 256), 1) // HEAD_DIM == iota((256, 256), 0) % 4
    spread = jnp.where(own_lanes, spread, 0.0)
    folded = spread[:, 0:128] + spread[:, 128:256]
    folded = folded + pltpu.roll(folded, 64, 1)
    query_rows[...] = folded
    wide = jnp.concatenate([folded] * 2, axis=1)
    block = iota((256, 256), 1) // HEAD_DIM == (iota((256, 256), 0) // 4) % 4
    left = jnp.where(block, wide * (HEAD_DIM ** (-0.5)), 0.0).astype(BF)

    me = lax.axis_index("kv")
    own_scale = scales[pl.ds(pl.multiple_of(8 * (me // 2), 8), 8), :]
    own_scale = jnp.where(me % 2 == 0, own_scale, pltpu.roll(own_scale, 4, 0))
    key_value = (own_scale * extra).astype(BF)
    forget = pltpu.roll(extra, 4, 0)
    forget = own_scale * (forget + pltpu.roll(forget, 124, 1))
    log_forget = -(jnp.maximum(-forget, 0.0) + jnp.log1p(jnp.exp(-jnp.abs(forget))))
    log_forget = jnp.where((iota((8, 128), 1) < 4) & (iota((8, 128), 0) < 4), log_forget, 0.0)
    repeat4 = iota((128, 8), 0) // 4 % 4 == iota((128, 8), 1)
    key_value = dot(repeat4.astype(BF), key_value)
    log_forget = jnp.dot(
        repeat4[0:16].astype(F32), log_forget, preferred_element_type=F32, precision=lax.Precision.HIGHEST
    )
    mine = iota((16, 128), 1) == iota((16, 128), 0) % 4
    log_forget = jnp.sum(jnp.where(mine, log_forget, 0.0), axis=1, keepdims=True)
    at = pl.ds(pl.multiple_of(16 * me, 16), 16)
    lower = iota((16, 128), 1) < 64
    own = jnp.sum(jnp.where(lower, query_rows[at, :] * key_value[0:16], 0.0), axis=1, keepdims=True)
    own = own * (HEAD_DIM ** (-0.5)) - log_forget
    own = jnp.concatenate([own] * 8, axis=0)
    place = iota((128, 128), 0) == iota((128, 128), 1)
    own = jnp.sum(jnp.where(place, own, 0.0), axis=0, keepdims=True)
    pick = (iota((64, 128), 1) == iota((64, 128), 0) + 64).astype(BF)
    value = dot_t(pick, key_value.astype(BF))

    lane = iota((64, 16), 1)
    folds = []
    def score(g):
        scores = dot(left[16 * g : 16 * g + 16], keys[256 * g : 256 * g + 256, :])
        return scores + decay[4 * g : 4 * g + 4].reshape(16, 1024)

    ahead = [score(g) for g in range(8)]
    for g in range(16):
        rows = slice(16 * g, 16 * g + 16)
        scores = ahead.pop(0)
        peak = jnp.max(scores, axis=1, keepdims=True)
        weights = jnp.exp(scores - peak)
        mass = jnp.sum(weights, axis=1, keepdims=True)
        peaks[rows, :] = jnp.broadcast_to(peak, (16, 128))
        masses[rows, :] = jnp.broadcast_to(mass, (16, 128))
        weights = weights.astype(BF)
        if g + 8 < 16:
            ahead.append(score(g + 8))
        summed = dot_t(values[256 * g : 256 * g + 256, :], weights)
        total = summed[0:64]
        for k in range(1, 4):
            total = jnp.where(lane // 4 == k, summed[64 * k : 64 * k + 64], total)
        folds.append(total)
    sums = [jnp.concatenate(folds[8 * j : 8 * j + 8], axis=1) for j in range(2)]

    line = iota((8, 128), 0)
    slot = iota((1, 128), 1) // 16
    packed = jnp.zeros((8, 128), F32)
    for j in range(2):
        rows = slice(128 * j, 128 * j + 128)
        peak = jnp.sum(jnp.where(place, peaks[rows, :], 0.0), axis=0, keepdims=True)
        mass = jnp.sum(jnp.where(place, masses[rows, :], 0.0), axis=0, keepdims=True)
        joined = jnp.where(slot + 8 * j == me, own, peak - 1e30)
        top = jnp.maximum(peak, joined)
        keep = jnp.exp(peak - top)
        weight = jnp.exp(joined - top)
        mass = mass * keep + weight
        result = ((sums[j] * keep + high(weight) * value) / mass).astype(BF)
        for i in range(16):
            out[i, 64 * j : 64 * j + 64, :] = result
        level = top + jnp.log(mass)
        for k in range(3):
            piece = high(level)
            packed = jnp.where(line == 3 * j + k, piece, packed)
            level = level - piece
    packed = packed.astype(BF)
    for i in range(16):
        out[i, 128:136, :] = packed


def merge_kernel(parts, w_out, out):
    extra = parts[:, 128:136, :].astype(F32)
    row, column = iota((128, 128), 0), iota((128, 128), 1)
    order = ((row % 32 == column // 4) & (row // 32 == column % 4)).astype(BF)
    heads = []
    for j in range(2):
        level = extra[:, 3 * j, :] + extra[:, 3 * j + 1, :] + extra[:, 3 * j + 2, :]
        factor = jnp.exp(level - jnp.max(level, axis=0, keepdims=True))
        factor = factor / jnp.sum(factor, axis=0, keepdims=True)
        total = [parts[i, 64 * j : 64 * j + 64, :].astype(F32) * factor[i : i + 1, :] for i in range(16)]
        while len(total) > 1:
            total = [a + b for a, b in zip(total[::2], total[1::2])]
        heads.append(dot_t(order, total[0].astype(BF)).astype(BF))
    partial = jnp.zeros((64, 256), F32)
    for h in range(4):
        attended = jnp.concatenate([heads[0][32 * h : 32 * h + 32], heads[1][32 * h : 32 * h + 32]], axis=0)
        partial = partial + dot(attended, w_out[64 * h : 64 * h + 64, :])
    out[...] = partial.astype(BF)


def pair_kernel(mine, partner, out):
    total = (mine[...].astype(F32) + partner[...].astype(F32)).astype(BF)
    for i in range(4):
        out[i] = total


def up_kernel(parts, tokens, gain, w_up, residual_out, out):
    attn = parts[0].astype(F32)
    for i in range(1, 4):
        attn = attn + parts[i].astype(F32)
    residual = (tokens[...].astype(F32) + high(attn)).astype(BF)
    residual_out[...] = residual
    wide = residual.astype(F32)
    squares = jnp.sum(wide * wide, axis=1, keepdims=True)
    squares_high = high(squares)
    row_high = column_to_row(squares_high, 128, 0)
    row_low = column_to_row(squares - squares_high, 128, 0)
    line = iota((8, 128), 0)
    tile = jnp.where(line == 0, row_high, jnp.where(line == 1, row_low, 0.0)).astype(BF)
    normed = (wide * gain[...]).astype(BF)
    for p in range(0, 16, 2):
        up = dot(normed, w_up[:, 128 * p : 128 * p + 256]).astype(BF)
        for k in range(2):
            out[p + k, 0:64, :] = up[:, 128 * k : 128 * k + 128]
            out[p + k, 64:72, :] = tile


def hidden_kernel(parts, out):
    total = [parts[i].astype(F32) for i in range(16)]
    while len(total) > 1:
        total = [a + b for a, b in zip(total[::2], total[1::2])]
    up, extra = total[0][0:64], total[0][64:72]
    squares = row_to_column(extra[0:1] + extra[1:2], 64, 0)
    up = lax.rsqrt(squares / D + EPS) * up
    up = jnp.maximum(up, 0.0)
    hidden = (up * up).astype(BF)
    for i in range(16):
        out[i] = hidden


def down_kernel(parts, w_down, out):
    down = jnp.zeros((64, 256), F32)
    for i in range(0, 16, 2):
        pair = jnp.concatenate([parts[i], parts[i + 1]], axis=1)
        down = down + dot(pair, w_down[128 * i : 128 * i + 256, :])
    out[...] = down.astype(BF)


def finish_kernel(parts, residual, out):
    down = parts[0].astype(F32)
    for i in range(1, 4):
        down = down + parts[i].astype(F32)
    out[...] = (residual[...].astype(F32) + high(down)).astype(BF)


def exchange(array, axis):
    return lax.all_to_all(array, axis, split_axis=0, concat_axis=0, tiled=True)


def pair_sum(partial):
    partner = lax.ppermute(partial, "core", [(0, 1), (1, 0)])
    message = call(pair_kernel, jax.ShapeDtypeStruct((4, 64, 256), BF), "pair")(partial, partner)
    return exchange(message, "x")


def attend(message, query_gain, key_cache, value_cache, decay_cache):
    return call(
        attend_kernel,
        jax.ShapeDtypeStruct((16, 136, 128), BF),
        "attend",
        scratch=[
            pltpu.VMEM((64, 128), F32),
            pltpu.VMEM((256, 128), F32),
            pltpu.VMEM((256, 128), F32),
            pltpu.VMEM((256, 128), F32),
        ],
        limit=8 << 20,
    )(
        message,
        query_gain.reshape(1, -1),
        key_cache.reshape(4096, 1024),
        value_cache.reshape(4096, 1024),
        decay_cache,
    )


def shards(
    tokens, mix_gain, w_query, w_key, w_value, w_forget, query_gain,
    key_cache, value_cache, decay_cache, w_out, mlp_gain, w_up, w_down,
):
    shape = jax.ShapeDtypeStruct
    head = call(head_kernel, shape((8, 128), F32), "head", cost=3 * 10**9)()
    operands = (tokens, mix_gain.reshape(1, -1), w_query, w_key.T, w_value.T, w_forget.T)
    query, extra = call(project_kernel, (shape((64, 256), BF), shape((128, 128), BF)), "project")(head, *operands)
    message = call(spread_kernel, shape((16, 136, 128), BF), "spread", cost=10**10)(query, extra)
    message = exchange(message, "kv")
    part = attend(message, query_gain, key_cache, value_cache, decay_cache)
    partial = call(merge_kernel, shape((64, 256), BF), "merge")(exchange(part, "kv"), w_out)
    residual, message = call(up_kernel, (shape((64, 256), BF), shape((16, 72, 128), BF)), "up")(
        pair_sum(partial), tokens, mlp_gain.reshape(1, -1), w_up
    )
    message = call(hidden_kernel, shape((16, 64, 128), BF), "hidden")(exchange(message, "kv"))
    partial = call(down_kernel, shape((64, 256), BF), "down")(exchange(message, "kv"), w_down)
    return call(finish_kernel, shape((64, 256), BF), "finish")(pair_sum(partial), residual)


def solution(mesh):
    split = Mesh(mesh.devices.reshape(mesh.shape["kv"], -1, 2), ("kv", "x", "core"))
    return jax.shard_map(
        shards,
        mesh=split,
        in_specs=(
            P(None, "kv"),
            P("kv"),
            P("kv", TP),
            P("kv", TP),
            P("kv", TP),
            P("kv", TP),
            P(),
            P(None, TP, None, "kv"),
            P(None, TP, None, "kv"),
            P(None, TP, "kv"),
            P(TP, "kv"),
            P("kv"),
            P("kv", TP),
            P(TP, "kv"),
        ),
        out_specs=P(None, "kv"),
        check_vma=False,
    )
```
